128 devices in a mesh: dp: 4 (over x), kv: 16 (over z, y), tp: 2 (over core).
Axes of the slice: x: 4, y: 4, z: 4, core: 2. Of those that a mesh axis runs over, the one named last changes fastest.
Arguments:
- tokens: bfloat16 [256, 4096], P('dp', 'kv'), may hold values from -6 to 6
- norm_gain: float32 [4096], P('kv'), may hold values from 0.1 to 1.9
- w_query: bfloat16 [4096, 2048], P('kv', 'tp'), may hold values from -0.09375 to 0.09375
- w_key: bfloat16 [4096, 2048], P('kv', 'tp'), may hold values from -0.09375 to 0.09375
- w_value: bfloat16 [4096, 2048], P('kv', 'tp'), may hold values from -0.09375 to 0.09375
- query_gain: float32 [64], replicated, may hold values from 0.1 to 1.9
- key_gain: float32 [64], replicated, may hold values from 0.1 to 1.9
- head_bias: float32 [32], P('tp'), may hold values from -11 to -3
- w_output: bfloat16 [2048, 4096], P('tp', 'kv'), may hold values from -0.125 to 0.125
- cache_keys: bfloat16 [16, 4096, 2048], P('dp', 'kv', 'tp'), may hold values from -6 to 6
- cache_values: bfloat16 [16, 4096, 2048], P('dp', 'kv', 'tp'), may hold values from -6 to 6
- base_length: int32 [16], P('dp'), may hold values from 3072 to 4064
- accepted: int32 [16], P('dp'), may hold values from 0 to 16
- parents: int32 [16, 16], P('dp'), may hold values from -1 to 14, as said below
Outputs:
- layer_out: bfloat16 [256, 4096], P('dp', 'kv')
- updated_keys: bfloat16 [16, 4096, 2048], P('dp', 'kv', 'tp')
- updated_values: bfloat16 [16, 4096, 2048], P('dp', 'kv', 'tp')
The draws below stay inside these ranges and needn't reach their ends.
Inputs may be any that keep to these rules, and one draw needn't show every extreme that they name: base_length + accepted + 16 <= 4096 for every sequence. parents[s, i] is -1 or a proposal before i; parents[s, 0] is -1.
All inputs are finite; a program needn't handle non-finite values.
Results may differ from the reference program's by a relative error of at most 0.00175.
The reference program's roundings to bfloat16 on the way count: a program that leaves them out, or rounds other values in their place, can miss the bound.
Values may be sent and summed in bfloat16 or wider, within the bound.
No kernel may reach another device: no remote copies, remote signals or barrier semaphores. Data moves between devices by JAX's collectives and lax.ppermute only.
A program may use at most 64 MiB of HBM per device.

```python
import jax
import jax.numpy as jnp
from jax import lax

D = 4096
HEADS = 32
HEAD_DIM = 64
PROP = 16
CACHE_DEV = 256
SEQS = 16
CACHE = 4096
ROWS = 256
QW = 2048
N_KV = 16


def draw_head_bias(key, part):
    pick_key, slow_key, fast_key = jax.random.split(key, 3)
    slow = jax.random.uniform(pick_key, (HEADS,)) < 0.5
    slow_value = jax.random.uniform(slow_key, (HEADS,), jnp.float32, -11.0, -8.0)
    fast_value = jax.random.uniform(fast_key, (HEADS,), jnp.float32, -4.5, -3.0)
    return jnp.where(slow, slow_value, fast_value).astype(jnp.float32)


def draw_cache_values(key, part):
    centre_key, noise_key = jax.random.split(key)
    centre = jax.random.normal(centre_key, (SEQS, 1, HEADS * HEAD_DIM), jnp.float32)
    noise = 0.5 * jax.random.normal(noise_key, (SEQS, CACHE, HEADS * HEAD_DIM), jnp.float32)
    return jnp.clip(centre + noise, -6.0, 6.0).astype(jnp.bfloat16)


def draw_parents(key, part):
    step_back = jax.random.randint(key, (SEQS, PROP), 1, 4)
    column = jnp.arange(PROP, dtype=jnp.int32)[None, :]
    step_back = jnp.where(column == PROP - 1, 1, step_back).astype(jnp.int32)
    return jnp.maximum(column - step_back, -1).astype(jnp.int32)


def touch_ends(entries, key, smallest, largest):
    longest = entries.shape.index(max(entries.shape))
    spots = []
    for shift in (0, 1):
        where = [jax.random.randint(jax.random.fold_in(key, axis), (), 0, length) for axis, length in enumerate(entries.shape)]
        where[longest] = (where[longest] + shift) % entries.shape[longest]
        spots.append(tuple(where))
    return entries.at[spots[0]].set(smallest).at[spots[1]].set(largest)


def level_of(rng, dims, cuts, low, high):
    factor_of = 1.0
    for axis_at, parts in cuts:
        heights = jax.random.uniform(jax.random.fold_in(jax.random.fold_in(rng, 6), axis_at), (parts,), jnp.float32, low / len(cuts), high / len(cuts))
        factor_of = factor_of * jnp.repeat(jnp.exp(heights), dims[axis_at] // parts).reshape((-1,) + (1,) * (len(dims) - 1 - axis_at))
    return factor_of


def normal_values(rng, extent, scale, reach, pieces=(), kind=jnp.bfloat16):
    loudness = level_of(rng, extent, pieces, -0.22, 0.18) if pieces else 1.0
    array = jax.random.normal(rng, extent, jnp.float32) * scale * loudness
    return jnp.minimum(jnp.maximum(array, -reach), reach).astype(kind)


def setup_inputs(seed: int = 0) -> dict:
    streams_of = jax.random.split(jax.random.key(seed), 15)
    tokens = normal_values(streams_of[0], (ROWS, D), 1.0, 6.0, ((0, 4), (1, 16)))
    norm_gain = jnp.clip(1.0 + 0.18 * jax.random.normal(streams_of[1], (D,), jnp.float32), 0.1, 1.9)
    w_query = normal_values(streams_of[2], (D, QW), D ** -0.5, 0.09375, ((0, 16), (1, 2)))
    w_key = normal_values(streams_of[3], (D, QW), D ** -0.5, 0.09375, ((0, 16), (1, 2)))
    w_value = normal_values(streams_of[4], (D, QW), D ** -0.5, 0.09375, ((0, 16), (1, 2)))
    query_gain = jnp.clip(1.0 + 0.18 * jax.random.normal(streams_of[5], (HEAD_DIM,), jnp.float32), 0.1, 1.9)
    key_gain = jnp.clip(1.0 + 0.18 * jax.random.normal(streams_of[6], (HEAD_DIM,), jnp.float32), 0.1, 1.9)
    head_bias = draw_head_bias(jax.random.fold_in(streams_of[14], 71), 0)
    w_output = normal_values(streams_of[8], (QW, D), QW ** -0.5, 0.125, ((0, 2), (1, 16)))
    cache_keys = normal_values(streams_of[9], (SEQS, CACHE, QW), 1.0, 6.0, ((0, 4), (1, 16), (2, 2)))
    cache_values = draw_cache_values(jax.random.fold_in(streams_of[14], 71), 0)
    base_length = touch_ends(jax.random.randint(streams_of[11], (SEQS,), CACHE - CACHE // 4, CACHE - 2 * PROP + 1), jax.random.fold_in(streams_of[11], 1), CACHE - CACHE // 4, CACHE - 2 * PROP).astype(jnp.int32)
    accepted = touch_ends(jax.random.randint(streams_of[12], (SEQS,), 0, PROP + 1), jax.random.fold_in(streams_of[12], 1), 0, PROP).astype(jnp.int32)
    parents = draw_parents(jax.random.fold_in(streams_of[14], 71), 0)
    return dict(tokens=tokens, norm_gain=norm_gain, w_query=w_query, w_key=w_key, w_value=w_value, query_gain=query_gain, key_gain=key_gain, head_bias=head_bias, w_output=w_output, cache_keys=cache_keys, cache_values=cache_values, base_length=base_length, accepted=accepted, parents=parents)


epsilon = 1e-05

def head_norm(raw, gain):
    grouped = raw.reshape(raw.shape[0], -1, gain.shape[0])
    factor = lax.rsqrt(lax.optimization_barrier(jnp.mean(grouped * grouped, axis=2, keepdims=True)) + epsilon)
    return (grouped * factor * gain).reshape(raw.shape).astype(jnp.bfloat16)

def ancestry(parents):
    width = parents.shape[-1]
    direct = (parents[..., :, None] == jnp.arange(width, dtype=jnp.int32)).astype(jnp.float32)

    def extend(step, above):
        return direct + jnp.einsum('sij,sjk->sik', direct, above)
    return lax.fori_loop(0, width - 1, extend, direct)

def attend_one(head_bias, inputs):
    query_heads, key_heads, value_heads, stored_keys, stored_values, visible_len, tree = inputs
    factor = HEAD_DIM ** (-0.5)
    query_wide = query_heads.astype(jnp.float32)
    stored_k = stored_keys.astype(jnp.float32).reshape(CACHE, HEADS, HEAD_DIM)
    stored_v = stored_values.astype(jnp.float32).reshape(N_KV, CACHE_DEV, HEADS, HEAD_DIM)
    score = jnp.einsum('qhd,phd->hqp', query_wide, stored_k) * factor + head_bias[:, None, None]
    live = jnp.arange(CACHE, dtype=jnp.int32) < visible_len
    stay = jnp.where(live, jax.nn.log_sigmoid(-score), 0.0)
    stay_blocks = stay.reshape(HEADS, PROP, N_KV, CACHE_DEV)
    taken = jax.nn.log_sigmoid(score).reshape(HEADS, PROP, N_KV, CACHE_DEV)
    tail = lax.cumsum(stay_blocks, axis=3, reverse=True) - stay_blocks
    weight = jnp.where(live.reshape(N_KV, CACHE_DEV), jnp.exp(taken + tail), 0.0).astype(jnp.bfloat16)
    block_sum = jnp.einsum('hqbc,bchd->qbhd', weight.astype(jnp.float32), stored_v)
    block_log = lax.optimization_barrier(jnp.sum(stay_blocks, axis=3))
    later = lax.cumsum(block_log, axis=2, reverse=True) - block_log
    cache_part = jnp.einsum('hqb,qbhd->qhd', jnp.exp(later), block_sum)
    inner = jnp.einsum('qhd,jhd->hqj', query_wide, key_heads.astype(jnp.float32)) * factor + head_bias[:, None, None]
    mine = tree > 0.5
    stay_tree = jnp.where(mine, jax.nn.log_sigmoid(-inner), 0.0)
    tail_tree = lax.cumsum(stay_tree, axis=2, reverse=True) - stay_tree
    weight_tree = jnp.where(mine, jnp.exp(jax.nn.log_sigmoid(inner) + tail_tree), 0.0).astype(jnp.bfloat16)
    ancestor_sum = jnp.einsum('hqj,jhd->qhd', weight_tree.astype(jnp.float32), value_heads.astype(jnp.float32))
    ancestor_log = lax.optimization_barrier(jnp.sum(stay_tree, axis=2))
    total = ancestor_sum + jnp.exp(ancestor_log).T[:, :, None] * cache_part
    return total.reshape(PROP, HEADS * HEAD_DIM)

def reference(tokens, norm_gain, w_query, w_key, w_value, query_gain, key_gain, head_bias, w_output, cache_keys, cache_values, base_length, accepted, parents):
    wide = tokens.astype(jnp.float32)
    scaled = (wide * norm_gain).astype(jnp.bfloat16)
    inv_rms = lax.rsqrt(lax.optimization_barrier(jnp.mean(wide * wide, axis=1)) + epsilon)
    query_raw = jnp.dot(scaled, w_query, preferred_element_type=jnp.float32)
    key_raw = jnp.dot(scaled, w_key, preferred_element_type=jnp.float32)
    value_raw = jnp.dot(scaled, w_value, preferred_element_type=jnp.float32)
    queries = head_norm(query_raw, query_gain)
    new_keys = head_norm(key_raw, key_gain)
    new_values = (value_raw * inv_rms[:, None]).astype(jnp.bfloat16)
    valid = (base_length + accepted).astype(jnp.int32)
    tree = ancestry(parents)
    seq_count = cache_keys.shape[0]
    shape_four = (seq_count, PROP, HEADS, HEAD_DIM)
    attended = lax.map(partial_attend(head_bias), (queries.reshape(shape_four), new_keys.reshape(shape_four), new_values.reshape(shape_four), cache_keys, cache_values, valid, tree))
    attended = attended.reshape(seq_count * PROP, HEADS * HEAD_DIM).astype(jnp.bfloat16)
    mix = jnp.dot(attended, w_output, preferred_element_type=jnp.float32)
    layer_out = (mix * lax.rsqrt(lax.optimization_barrier(jnp.mean(mix * mix, axis=1, keepdims=True)) + epsilon)).astype(jnp.bfloat16)

    def write(stored, fresh, start):
        return lax.dynamic_update_slice_in_dim(stored, fresh, start, axis=0)
    updated_keys = jax.vmap(write)(cache_keys, new_keys.reshape(seq_count, PROP, -1), valid)
    updated_values = jax.vmap(write)(cache_values, new_values.reshape(seq_count, PROP, -1), valid)
    return (layer_out, updated_keys, updated_values)

def partial_attend(head_bias):

    def apply(inputs):
        return attend_one(head_bias, inputs)
    return apply
```

```python
import functools

import jax
import jax.numpy as jnp
from jax import lax
from jax.experimental import pallas as pl
from jax.experimental.pallas import tpu as pltpu
from jax.sharding import Mesh
from jax.sharding import PartitionSpec as P

HEAD_DIM = 64
LANES = 128
KV = ("kv_0", "kv_1")
MIB = 1 << 20

epsilon = 1e-05
f32 = jnp.float32
bf16 = jnp.bfloat16


def low_half(rows):
    return lax.broadcasted_iota(jnp.int32, (rows, LANES), 1) < HEAD_DIM


def turned(x):
    return pltpu.roll(x, HEAD_DIM, 1)


def dot(a, b):
    return jnp.dot(a, b, preferred_element_type=f32)


def dot_nt(a, b):
    return lax.dot_general(a, b, (((1,), (1,)), ((), ())), preferred_element_type=f32)


def split_bf16(x, pieces):
    parts = []
    for _ in range(pieces):
        part = x.astype(bf16)
        parts.append(part)
        x = x - part.astype(f32)
    return parts


def signs(z):
    spill = jnp.log(1.0 + jnp.exp(-jnp.abs(z)))
    return -jnp.maximum(z, 0.0) - spill, jnp.minimum(z, 0.0) - spill


def project_kernel(tokens, gain, w_query, w_key, w_value, slots):
    rows, half = tokens.shape[0], tokens.shape[0] // 2
    wide = tokens[...].astype(f32)
    scaled = (wide * gain[...]).astype(bf16)
    low, low_v = low_half(rows), low_half(half)
    for at in range(0, w_query.shape[1], 2 * LANES):
        columns = pl.ds(at, 2 * LANES)
        query = dot(scaled, w_query[:, columns])
        key = dot(scaled, w_key[:, columns])
        value = dot(scaled, w_value[:, columns])
        for tile in range(2):
            head = at // HEAD_DIM + 2 * tile
            lanes = slice(tile * LANES, (tile + 1) * LANES)
            q, k, v = query[:, lanes], turned(key[:, lanes]), value[:, lanes]
            v_turned = turned(v)
            slots[head, :rows] = jnp.where(low, q, k)
            slots[head + 1, :rows] = jnp.where(low, k, q)
            slots[head, rows : rows + half] = jnp.where(low_v, v[:half], v_turned[half:])
            slots[head + 1, rows : rows + half] = jnp.where(low_v, v_turned[:half], v[half:])
    squares = wide * wide
    squares = jnp.concatenate((squares, jnp.zeros((LANES - rows, squares.shape[1]), f32)), axis=0)
    ones = jnp.ones((8, squares.shape[1]), bf16)
    row_squares = sum(dot_nt(ones, part) for part in split_bf16(squares, 3))
    for head in range(slots.shape[0]):
        slots[head, rows + half :] = row_squares


def normalize_kernel(width, place, got, query_gain, key_gain, slots, own):
    peers = got.shape[0]
    rows = got.shape[1] - 8
    half = rows // 3
    rows = 2 * half
    even = place[0] % 2 == 0
    total = got[0]
    for peer in range(1, peers):
        total = total + got[peer]
    both, value, squares = total[:rows], total[rows : rows + half], total[rows + half : rows + half + 1]
    low = low_half(rows)
    power = both * both
    low_sum = jnp.sum(jnp.where(low, power, 0.0), axis=1, keepdims=True)
    high_sum = jnp.sum(jnp.where(low, 0.0, power), axis=1, keepdims=True)
    factor = lax.rsqrt(jnp.where(low, low_sum, high_sum) / HEAD_DIM + epsilon)
    low_gain = jnp.where(even, query_gain[...], key_gain[...])
    high_gain = jnp.where(even, key_gain[...], query_gain[...])
    normed = (both * factor * jnp.where(low, low_gain, high_gain)).astype(bf16)
    inv_rms = jnp.broadcast_to(lax.rsqrt(squares / width + epsilon), (half, LANES))
    lane = lax.broadcasted_iota(jnp.int32, (half, LANES), 1)
    row = lax.broadcasted_iota(jnp.int32, (half, LANES), 0)
    first = jnp.sum(jnp.where(lane == row, inv_rms, 0.0), axis=1, keepdims=True)
    second = jnp.sum(jnp.where(lane == row + half, inv_rms, 0.0), axis=1, keepdims=True)
    fresh = (value * jnp.where(lane < HEAD_DIM, first, second)).astype(bf16)
    own[:rows] = normed
    own[rows:] = fresh
    for peer in range(peers):
        slots[peer, :rows] = normed
        slots[peer, rows:] = fresh


def tree_kernel(prop, place, bias, own, parents, out):
    half = own.shape[0] // 3
    rows = 2 * half
    even = place[0] % 2 == 0
    low = low_half(rows)
    both = own[:rows].astype(f32)
    other = turned(both)
    query = jnp.where(low, jnp.where(even, both, other), 0.0).astype(bf16)
    key = jnp.where(even, other, both).astype(bf16)
    score = dot_nt(query, key) * HEAD_DIM ** (-0.5) + bias[place[0]]
    row = lax.broadcasted_iota(jnp.int32, (rows, rows), 0)
    column = lax.broadcasted_iota(jnp.int32, (rows, rows), 1)
    parent = parents[...]
    direct = (parent >= 0) & (column == row - row % prop + parent)
    step = jnp.where(direct, 1.0, 0.0).astype(bf16)
    above = jnp.where(row == column, 1.0, 0.0)
    above = above + step.astype(f32)
    reach = 2
    while reach < prop:
        step = dot(step, step).astype(bf16)
        above = above + dot(above.astype(bf16), step)
        reach *= 2
    mine = (above > 0.5) & (row != column)
    stay, taken = signs(score)
    stay = jnp.where(mine, stay, 0.0)
    after = jnp.where(row > column, 1.0, 0.0).astype(bf16)
    tail = sum(dot(part, after) for part in split_bf16(stay, 3))
    weight = jnp.where(mine, jnp.exp(taken + tail), 0.0).astype(bf16)
    kept = jnp.exp(jnp.sum(stay, axis=1, keepdims=True))
    value = own[rows:].astype(f32)
    value = jnp.concatenate((value, turned(value)), axis=0).astype(bf16)
    summed = dot(weight, value)
    low = low_half(half)
    out[0] = jnp.where(low, summed[:half], turned(summed[half:]))
    out[1] = jnp.where(low, kept[:half], kept[half:])


def attend_kernel(prop, place, valid, bias, fresh, keys, values, slots):
    seqs, span, _ = keys.shape
    heads = fresh.shape[0]
    rows = seqs * prop
    group = 4
    tall = heads * prop
    low = low_half(prop)
    low_mask = low.astype(f32).astype(bf16)
    high_mask = (1.0 - low.astype(f32)).astype(bf16)
    blank = jnp.zeros((prop, LANES), bf16)
    order = lax.broadcasted_iota(jnp.int32, (span, span), 0)
    after = jnp.where(order > lax.broadcasted_iota(jnp.int32, (span, span), 1), 1.0, 0.0).astype(bf16)
    position = place[0] * span + lax.broadcasted_iota(jnp.int32, (1, span), 1)
    quarter = lax.broadcasted_iota(jnp.int32, (prop, LANES), 1) // (LANES // seqs)
    sums, logs = [], []
    for seq in range(seqs):
        live = position < valid[seq]
        scores = []
        for first in range(0, heads, group):
            blocks = []
            for j in range(group):
                tile = fresh[first + j, seq * prop : (seq + 1) * prop] * (low_mask if j % 2 == 0 else high_mask)
                blocks.append(jnp.concatenate((tile, blank) if j < 2 else (blank, tile), axis=1))
            stored = keys[seq, :, first * HEAD_DIM : (first + group) * HEAD_DIM]
            score = dot_nt(jnp.concatenate(blocks, axis=0), stored)
            for j in range(group):
                part = score[j * prop : (j + 1) * prop]
                scores.append(part * HEAD_DIM ** (-0.5) + bias[first + j])
        stay, taken = signs(jnp.concatenate(scores, axis=0))
        stay = jnp.where(live, stay, 0.0)
        tail = dot(jnp.concatenate(split_bf16(stay, 2), axis=0), after)
        tail = tail[:tall] + tail[tall:]
        weight = jnp.where(live, jnp.exp(taken + tail), 0.0).astype(bf16)
        logs.append(tail[:, :1] + stay[:, :1])
        tiles = []
        for first in range(0, heads, group):
            stored = values[seq, :, first * HEAD_DIM : (first + group) * HEAD_DIM]
            summed = dot(weight[first * prop : (first + group) * prop], stored)
            for j in range(group):
                lanes = slice(j // 2 * LANES, (j // 2 + 1) * LANES)
                tiles.append(summed[j * prop : (j + 1) * prop, lanes])
        sums.append(tiles)
    for head in range(heads):
        for seq in range(seqs // 2):
            one, two = sums[seq][head], sums[seq + seqs // 2][head]
            one, two = (one, turned(two)) if head % 2 == 0 else (turned(one), two)
            slots[head, seq * prop : (seq + 1) * prop] = jnp.where(low, one, two)
        log = jnp.zeros((prop, LANES), f32)
        for seq in range(seqs):
            log = jnp.where(quarter == seq, logs[seq][head * prop : (head + 1) * prop], log)
        slots[head, rows // 2 :] = log


def combine_kernel(got, tree, slots):
    blocks, tall, _ = got.shape
    prop = tall // 3
    half = 2 * prop
    lane = lax.broadcasted_iota(jnp.int32, (prop, LANES), 1)
    first = lane % HEAD_DIM < HEAD_DIM // 2
    later = jnp.zeros((prop, LANES), f32)
    part = jnp.zeros((half, LANES), f32)
    for block in range(blocks - 1, -1, -1):
        kept = jnp.exp(later)
        one = jnp.where(first, kept, pltpu.roll(kept, HEAD_DIM // 2, 1))
        two = jnp.where(first, pltpu.roll(kept, LANES - HEAD_DIM // 2, 1), kept)
        part = part + jnp.concatenate((one, two), axis=0) * got[block, :half]
        later = later + got[block, half:]
    attended = (tree[0] + tree[1] * part).astype(bf16)
    for block in range(blocks):
        slots[block] = attended


def output_kernel(got, w_output, out):
    heads, half, _ = got.shape
    low = low_half(half)
    columns = []
    for head in range(0, heads, 2):
        one, two = got[head].astype(f32), got[head + 1].astype(f32)
        top = jnp.where(low, one, turned(two))
        bottom = jnp.where(low, turned(one), two)
        columns.append(jnp.concatenate((top, bottom), axis=0).astype(bf16))
    out[...] = dot(jnp.concatenate(columns, axis=1), w_output[...])


def squares_kernel(one, two, mix, slots):
    total = one[...] + two[...]
    mix[...] = total
    rows = total.shape[0]
    squares = jnp.sum(total * total, axis=1, keepdims=True)
    lane = lax.broadcasted_iota(jnp.int32, (rows, LANES), 1)
    row = lax.broadcasted_iota(jnp.int32, (rows, LANES), 0)
    flat = jnp.sum(jnp.where(lane == row, squares, 0.0), axis=0, keepdims=True)
    slots[...] = jnp.broadcast_to(flat[None], slots.shape)


def finish_kernel(width, mix, got, out):
    total = got[0]
    for peer in range(1, got.shape[0]):
        total = total + got[peer]
    rows = out.shape[0]
    factor = jnp.broadcast_to(lax.rsqrt(total[:1] / width + epsilon), (rows, LANES))
    lane = lax.broadcasted_iota(jnp.int32, (rows, LANES), 1)
    row = lax.broadcasted_iota(jnp.int32, (rows, LANES), 0)
    factor = jnp.sum(jnp.where(lane == row, factor, 0.0), axis=1, keepdims=True)
    out[...] = (mix[...] * factor).astype(bf16)


def update_kernel(prop, place, valid, fresh, keys, values, new_keys, new_values):
    seq = pl.program_id(0)
    _, span, _ = keys.shape
    heads = fresh.shape[0]
    rows = 2 * (fresh.shape[1] // 3)
    ahead = place[0] * span - valid[seq]
    new_keys[...] = keys[...]
    new_values[...] = values[...]

    @pl.when((ahead > -span) & (ahead < prop))
    def _():
        low = low_half(prop)
        early = seq < rows // prop // 2
        key_rows = pl.ds(pl.multiple_of(seq * prop, prop), prop)
        value_rows = pl.ds(pl.multiple_of(rows + seq % (rows // prop // 2) * prop, prop), prop)
        key_tiles, value_tiles = [], []
        for head in range(0, heads, 2):
            one, two = fresh[head, key_rows].astype(f32), fresh[head + 1, key_rows].astype(f32)
            key_tiles.append(turned(jnp.where(low, two, one)))
            one, two = fresh[head, value_rows].astype(f32), fresh[head + 1, value_rows].astype(f32)
            one = jnp.where(early, one, turned(one))
            two = jnp.where(early, turned(two), two)
            value_tiles.append(jnp.where(low, one, two))
        offset = ahead + lax.broadcasted_iota(jnp.int32, (span, prop), 0)
        chooser = jnp.where(offset == lax.broadcasted_iota(jnp.int32, (span, prop), 1), 1.0, 0.0).astype(bf16)
        offset = ahead + lax.broadcasted_iota(jnp.int32, (span, 1), 0)
        inside = (offset >= 0) & (offset < prop)
        for tiles, old, new in ((key_tiles, keys, new_keys), (value_tiles, values, new_values)):
            placed = dot(chooser, jnp.concatenate(tiles, axis=1).astype(bf16))
            new[0] = jnp.where(inside, placed, old[0].astype(f32)).astype(bf16)


VMEM = pl.BlockSpec(memory_space=pltpu.VMEM)
SMEM = pl.BlockSpec(memory_space=pltpu.SMEM)


def call(body, outs, specs, flops, moved, limit):
    return pl.pallas_call(
        body,
        out_shape=outs,
        in_specs=specs,
        out_specs=jax.tree.map(lambda _: VMEM, outs),
        cost_estimate=pl.CostEstimate(flops=flops, bytes_accessed=moved, transcendentals=0),
        compiler_params=pltpu.CompilerParams(vmem_limit_bytes=limit * MIB),
    )


def shape(*dims, dtype=f32):
    return jax.ShapeDtypeStruct(dims, dtype)


def exchanged(slots, axis):
    return lax.all_to_all(slots, axis, 0, 0, tiled=True)


def shards(
    tokens,
    norm_gain,
    w_query,
    w_key,
    w_value,
    query_gain,
    key_gain,
    head_bias,
    w_output,
    cache_keys,
    cache_values,
    base_length,
    accepted,
    parents,
):
    seqs, prop = parents.shape
    heads = head_bias.shape[0]
    rows, span = seqs * prop, cache_keys.shape[1]
    half = rows // 2
    columns = w_output.shape[1]
    peers = lax.axis_size(KV)
    width = tokens.shape[1] * peers
    assert peers == heads and seqs == 4 and rows <= LANES and heads % 4 == 0 and prop == 16
    place = lax.axis_index(KV).astype(jnp.int32).reshape(1)
    valid = base_length + accepted
    parent_column = parents.reshape(rows, 1)
    gains = [jnp.concatenate((g, g)).reshape(1, LANES) for g in (query_gain, key_gain)]

    slots = call(
        project_kernel,
        shape(heads, rows + half + 8, LANES),
        [VMEM] * 5,
        10**8,
        3 * MIB,
        12,
    )(tokens, norm_gain.reshape(1, -1), w_query, w_key, w_value)
    got = exchanged(slots, KV)
    slots, own = call(
        functools.partial(normalize_kernel, width),
        (shape(peers, rows + half, LANES, dtype=bf16), shape(rows + half, LANES, dtype=bf16)),
        [SMEM, VMEM, VMEM, VMEM],
        10**7,
        MIB,
        8,
    )(place, got, *gains)
    fresh = exchanged(slots, KV)
    tree = call(
        functools.partial(tree_kernel, prop),
        shape(2, half, LANES),
        [SMEM, SMEM, VMEM, VMEM],
        10**7,
        MIB // 8,
        8,
    )(place, head_bias, own, parent_column)
    slots = call(
        functools.partial(attend_kernel, prop),
        shape(heads, half + prop, LANES),
        [SMEM, SMEM, SMEM, VMEM, VMEM, VMEM],
        4 * 10**8,
        5 * MIB,
        24,
    )(place, valid, head_bias, fresh, cache_keys, cache_values)
    got = exchanged(slots, KV)
    block = pl.BlockSpec((1, span, cache_keys.shape[2]), lambda s: (s, 0, 0))
    updated_keys, updated_values = pl.pallas_call(
        functools.partial(update_kernel, prop),
        grid=(seqs,),
        out_shape=(cache_keys, cache_values),
        in_specs=[SMEM, SMEM, VMEM, block, block],
        out_specs=(block, block),
        cost_estimate=pl.CostEstimate(flops=10**8, bytes_accessed=8 * MIB, transcendentals=0),
        compiler_params=pltpu.CompilerParams(vmem_limit_bytes=16 * MIB),
    )(place, valid, fresh, cache_keys, cache_values)
    slots = call(combine_kernel, shape(peers, half, LANES, dtype=bf16), [VMEM] * 2, 10**7, MIB, 8)(got, tree)
    got = exchanged(slots, KV)
    part = call(output_kernel, shape(rows, columns), [VMEM] * 2, 10**8, MIB, 8)(got, w_output)
    other = lax.ppermute(part, "tp", [(0, 1), (1, 0)])
    mix, slots = call(
        squares_kernel, (shape(rows, columns), shape(peers, 8, LANES)), [VMEM] * 2, 10**6, MIB // 4, 4
    )(part, other)
    got = exchanged(slots, KV)
    layer_out = call(
        functools.partial(finish_kernel, columns * peers),
        shape(rows, columns, dtype=bf16),
        [VMEM] * 2,
        10**6,
        MIB // 8,
        4,
    )(mix, got)
    return (layer_out, updated_keys, updated_values)


def solution(mesh):
    finer = Mesh(
        mesh.devices.reshape(mesh.shape["dp"], 4, 4, mesh.shape["tp"]), ("dp", "kv_0", "kv_1", "tp")
    )
    return jax.shard_map(
        shards,
        mesh=finer,
        in_specs=(
            P("dp", KV),
            P(KV),
            P(KV, "tp"),
            P(KV, "tp"),
            P(KV, "tp"),
            P(),
            P(),
            P("tp"),
            P("tp", KV),
            P("dp", KV, "tp"),
            P("dp", KV, "tp"),
            P("dp"),
            P("dp"),
            P("dp", None),
        ),
        out_specs=(P("dp", KV), P("dp", KV, "tp"), P("dp", KV, "tp")),
        check_vma=False,
    )
```

```python
import functools

import jax
import jax.numpy as jnp
from jax import lax
from jax.experimental import pallas as pl
from jax.experimental.pallas import tpu as pltpu
from jax.sharding import Mesh
from jax.sharding import PartitionSpec as P

HEAD_DIM = 64
LANES = 128
KV = ("kv_0", "kv_1")
MIB = 1 << 20

epsilon = 1e-05
f32 = jnp.float32
bf16 = jnp.bfloat16


def low_half(rows):
    return lax.broadcasted_iota(jnp.int32, (rows, LANES), 1) < HEAD_DIM


def turned(x):
    return pltpu.roll(x, HEAD_DIM, 1)


def dot(a, b):
    return jnp.dot(a, b, preferred_element_type=f32)


def dot_nt(a, b):
    return lax.dot_general(a, b, (((1,), (1,)), ((), ())), preferred_element_type=f32)


def split_bf16(x, pieces):
    parts = []
    for _ in range(pieces):
        part = x.astype(bf16)
        parts.append(part)
        x = x - part.astype(f32)
    return parts


def signs(z):
    spill = jnp.log(1.0 + jnp.exp(-jnp.abs(z)))
    return -jnp.maximum(z, 0.0) - spill, jnp.minimum(z, 0.0) - spill


def project_kernel(*refs):
    sources, slots, (tokens, gain, w_query, w_key, w_value), arrived = refs[:5], refs[5], refs[6:11], refs[11]
    copies = [
        pltpu.make_async_copy(source, held, arrived.at[at])
        for at, (source, held) in enumerate(zip(sources, refs[6:11]))
    ]
    for copy in copies:
        copy.start()
    rows, half = tokens.shape[0], tokens.shape[0] // 2
    low, low_v = low_half(rows), low_half(half)
    copies[0].wait()
    wide = tokens[...].astype(f32)
    squares = wide * wide
    squares = jnp.concatenate((squares, jnp.zeros((LANES - rows, squares.shape[1]), f32)), axis=0)
    ones = jnp.ones((8, squares.shape[1]), bf16)
    row_squares = sum(dot_nt(ones, part) for part in split_bf16(squares, 3))
    for head in range(slots.shape[0]):
        slots[head, rows + half :] = row_squares
    copies[1].wait()
    scaled = (wide * gain[...]).astype(bf16)
    copies[2].wait()
    copies[3].wait()
    spans = [pl.ds(at, 2 * LANES) for at in range(0, w_query.shape[1], 2 * LANES)]
    tiles = [slice(0, LANES), slice(LANES, 2 * LANES)]
    for at, columns in enumerate(spans):
        query, key = dot(scaled, w_query[:, columns]), dot(scaled, w_key[:, columns])
        for tile, lanes in enumerate(tiles):
            head = 4 * at + 2 * tile
            q, k = query[:, lanes], turned(key[:, lanes])
            slots[head, :rows] = jnp.where(low, q, k)
            slots[head + 1, :rows] = jnp.where(low, k, q)
    copies[4].wait()
    for at, columns in enumerate(spans):
        value = dot(scaled, w_value[:, columns])
        for tile, lanes in enumerate(tiles):
            head = 4 * at + 2 * tile
            v = value[:, lanes]
            v_turned = turned(v)
            slots[head, rows : rows + half] = jnp.where(low_v, v[:half], v_turned[half:])
            slots[head + 1, rows : rows + half] = jnp.where(low_v, v_turned[:half], v[half:])


def normalize_kernel(width, got, query_gain, key_gain, slots, own):
    peers = got.shape[0]
    rows = got.shape[1] - 8
    half = rows // 3
    rows = 2 * half
    even = lax.axis_index(KV) % 2 == 0
    total = got[0]
    for peer in range(1, peers):
        total = total + got[peer]
    both, value, squares = total[:rows], total[rows : rows + half], total[rows + half : rows + half + 1]
    low = low_half(rows)
    power = both * both
    low_sum = jnp.sum(jnp.where(low, power, 0.0), axis=1, keepdims=True)
    high_sum = jnp.sum(jnp.where(low, 0.0, power), axis=1, keepdims=True)
    factor = lax.rsqrt(jnp.where(low, low_sum, high_sum) / HEAD_DIM + epsilon)
    one, two = query_gain[...], key_gain[...]
    gain = jnp.concatenate((jnp.where(even, one, two), jnp.where(even, two, one)), axis=1)
    normed = (both * factor * gain).astype(bf16)
    inv_rms = jnp.broadcast_to(lax.rsqrt(squares / width + epsilon), (half, LANES))
    lane = lax.broadcasted_iota(jnp.int32, (half, LANES), 1)
    row = lax.broadcasted_iota(jnp.int32, (half, LANES), 0)
    first = jnp.sum(jnp.where(lane == row, inv_rms, 0.0), axis=1, keepdims=True)
    second = jnp.sum(jnp.where(lane == row + half, inv_rms, 0.0), axis=1, keepdims=True)
    fresh = (value * jnp.where(lane < HEAD_DIM, first, second)).astype(bf16)
    own[:rows] = normed
    own[rows:] = fresh
    for peer in range(peers):
        slots[peer, :rows] = normed
        slots[peer, rows:] = fresh


def tree_part(prop, bias, own, parents, out):
    half = own.shape[0] // 3
    rows = 2 * half
    even = lax.axis_index(KV) % 2 == 0
    low = low_half(rows)
    both = own[:rows].astype(f32)
    other = turned(both)
    query = jnp.where(low, jnp.where(even, both, other), 0.0).astype(bf16)
    key = jnp.where(even, other, both).astype(bf16)
    score = dot_nt(query, key) * HEAD_DIM ** (-0.5) + bias[lax.axis_index(KV)]
    row = lax.broadcasted_iota(jnp.int32, (rows, rows), 0)
    column = lax.broadcasted_iota(jnp.int32, (rows, rows), 1)
    small = [lax.broadcasted_iota(jnp.int32, (prop, prop), axis) for axis in range(2)]
    parent = jnp.concatenate(
        [
            jnp.sum(jnp.where(small[0] == small[1], parents[seq : seq + 1], 0), axis=1, keepdims=True)
            for seq in range(rows // prop)
        ],
        axis=0,
    )
    direct = (parent >= 0) & (column == row - row % prop + parent)
    step = jnp.where(direct, 1.0, 0.0).astype(bf16)
    above = jnp.where(row == column, 1.0, 0.0)
    above = above + step.astype(f32)
    reach = 2
    while reach < prop:
        step = dot(step, step).astype(bf16)
        above = above + dot(above.astype(bf16), step)
        reach *= 2
    mine = (above > 0.5) & (row != column)
    stay, taken = signs(score)
    stay = jnp.where(mine, stay, 0.0)
    after = jnp.where(row > column, 1.0, 0.0).astype(bf16)
    tail = sum(dot(part, after) for part in split_bf16(stay, 3))
    weight = jnp.where(mine, jnp.exp(taken + tail), 0.0).astype(bf16)
    kept = jnp.exp(jnp.sum(stay, axis=1, keepdims=True))
    value = own[rows:].astype(f32)
    value = jnp.concatenate((value, turned(value)), axis=0).astype(bf16)
    summed = dot(weight, value)
    low = low_half(half)
    out[0] = jnp.where(low, summed[:half], turned(summed[half:]))
    out[1] = jnp.where(low, kept[:half], kept[half:])


def attend_kernel(prop, base, accepted, bias, fresh, keys, values, slots):
    seqs, span, _ = keys.shape
    heads = fresh.shape[0]
    rows = seqs * prop
    group = 4
    tall = heads * prop
    low = low_half(prop)
    low_mask = low.astype(f32).astype(bf16)
    high_mask = (1.0 - low.astype(f32)).astype(bf16)
    blank = jnp.zeros((prop, LANES), bf16)
    order = lax.broadcasted_iota(jnp.int32, (span, span), 0)
    after = jnp.where(order > lax.broadcasted_iota(jnp.int32, (span, span), 1), 1.0, 0.0).astype(bf16)
    position = lax.axis_index(KV) * span + lax.broadcasted_iota(jnp.int32, (1, span), 1)
    quarter = lax.broadcasted_iota(jnp.int32, (prop, LANES), 1) // (LANES // seqs)
    sums, logs = [], []
    for seq in range(seqs):
        live = position < base[seq] + accepted[seq]
        scores = []
        for first in range(0, heads, group):
            blocks = []
            for j in range(group):
                tile = fresh[first + j, seq * prop : (seq + 1) * prop] * (low_mask if j % 2 == 0 else high_mask)
                blocks.append(jnp.concatenate((tile, blank) if j < 2 else (blank, tile), axis=1))
            stored = keys[seq, :, first * HEAD_DIM : (first + group) * HEAD_DIM]
            score = dot_nt(jnp.concatenate(blocks, axis=0), stored)
            for j in range(group):
                part = score[j * prop : (j + 1) * prop]
                scores.append(part * HEAD_DIM ** (-0.5) + bias[first + j])
        stay, taken = signs(jnp.concatenate(scores, axis=0))
        stay = jnp.where(live, stay, 0.0)
        tail = dot(jnp.concatenate(split_bf16(stay, 2), axis=0), after)
        tail = tail[:tall] + tail[tall:]
        weight = jnp.where(live, jnp.exp(taken + tail), 0.0).astype(bf16)
        logs.append(tail[:, :1] + stay[:, :1])
        tiles = []
        for first in range(0, heads, group):
            stored = values[seq, :, first * HEAD_DIM : (first + group) * HEAD_DIM]
            summed = dot(weight[first * prop : (first + group) * prop], stored)
            for j in range(group):
                lanes = slice(j // 2 * LANES, (j // 2 + 1) * LANES)
                tiles.append(summed[j * prop : (j + 1) * prop, lanes])
        sums.append(tiles)
    for head in range(heads):
        for seq in range(seqs // 2):
            one, two = sums[seq][head], sums[seq + seqs // 2][head]
            one, two = (one, turned(two)) if head % 2 == 0 else (turned(one), two)
            slots[head, seq * prop : (seq + 1) * prop] = jnp.where(low, one, two)
        log = jnp.zeros((prop, LANES), f32)
        for seq in range(seqs):
            log = jnp.where(quarter == seq, logs[seq][head * prop : (head + 1) * prop], log)
        slots[head, rows // 2 :] = log


def combine_kernel(got, tree, slots):
    blocks, tall, _ = got.shape
    prop = tall // 3
    half = 2 * prop
    lane = lax.broadcasted_iota(jnp.int32, (prop, LANES), 1)
    first = lane % HEAD_DIM < HEAD_DIM // 2
    later = jnp.zeros((prop, LANES), f32)
    part = jnp.zeros((half, LANES), f32)
    for block in range(blocks - 1, -1, -1):
        kept = jnp.exp(later)
        one = jnp.where(first, kept, pltpu.roll(kept, HEAD_DIM // 2, 1))
        two = jnp.where(first, pltpu.roll(kept, LANES - HEAD_DIM // 2, 1), kept)
        part = part + jnp.concatenate((one, two), axis=0) * got[block, :half]
        later = later + got[block, half:]
    attended = (tree[0] + tree[1] * part).astype(bf16)
    for block in range(blocks):
        slots[block] = attended


def output_kernel(got, w_output, out):
    heads, half, _ = got.shape
    low = low_half(half)
    columns = []
    for head in range(0, heads, 2):
        one, two = got[head].astype(f32), got[head + 1].astype(f32)
        top = jnp.where(low, one, turned(two))
        bottom = jnp.where(low, turned(one), two)
        columns.append(jnp.concatenate((top, bottom), axis=0).astype(bf16))
    out[...] = dot(jnp.concatenate(columns, axis=1), w_output[...])


def squares_kernel(one, two, mix, slots):
    total = one[...] + two[...]
    mix[...] = total
    rows = total.shape[0]
    squares = jnp.sum(total * total, axis=1, keepdims=True)
    lane = lax.broadcasted_iota(jnp.int32, (rows, LANES), 1)
    row = lax.broadcasted_iota(jnp.int32, (rows, LANES), 0)
    flat = jnp.sum(jnp.where(lane == row, squares, 0.0), axis=0, keepdims=True)
    slots[...] = jnp.broadcast_to(flat[None], slots.shape)


def finish_kernel(width, mix, got, out):
    total = got[0]
    for peer in range(1, got.shape[0]):
        total = total + got[peer]
    rows = out.shape[0]
    factor = jnp.broadcast_to(lax.rsqrt(total[:1] / width + epsilon), (rows, LANES))
    lane = lax.broadcasted_iota(jnp.int32, (rows, LANES), 1)
    row = lax.broadcasted_iota(jnp.int32, (rows, LANES), 0)
    factor = jnp.sum(jnp.where(lane == row, factor, 0.0), axis=1, keepdims=True)
    out[...] = (mix[...] * factor).astype(bf16)


def side_kernel(prop, base, accepted, bias, own, parents, fresh, keys, values, tree, new_keys, new_values):
    seq = pl.program_id(0)
    _, span, _ = keys.shape
    heads = fresh.shape[0]
    rows = 2 * (fresh.shape[1] // 3)
    ahead = lax.axis_index(KV) * span - base[seq] - accepted[seq]
    pl.when(seq == 0)(functools.partial(tree_part, prop, bias, own, parents, tree))
    new_keys[...] = keys[...]
    new_values[...] = values[...]

    @pl.when((ahead > -span) & (ahead < prop))
    def _():
        low = low_half(prop)
        early = seq < rows // prop // 2
        key_rows = pl.ds(pl.multiple_of(seq * prop, prop), prop)
        value_rows = pl.ds(pl.multiple_of(rows + seq % (rows // prop // 2) * prop, prop), prop)
        key_tiles, value_tiles = [], []
        for head in range(0, heads, 2):
            one, two = fresh[head, key_rows].astype(f32), fresh[head + 1, key_rows].astype(f32)
            key_tiles.append(turned(jnp.where(low, two, one)))
            one, two = fresh[head, value_rows].astype(f32), fresh[head + 1, value_rows].astype(f32)
            one = jnp.where(early, one, turned(one))
            two = jnp.where(early, turned(two), two)
            value_tiles.append(jnp.where(low, one, two))
        offset = ahead + lax.broadcasted_iota(jnp.int32, (span, prop), 0)
        chooser = jnp.where(offset == lax.broadcasted_iota(jnp.int32, (span, prop), 1), 1.0, 0.0).astype(bf16)
        offset = ahead + lax.broadcasted_iota(jnp.int32, (span, 1), 0)
        inside = (offset >= 0) & (offset < prop)
        for tiles, old, new in ((key_tiles, keys, new_keys), (value_tiles, values, new_values)):
            placed = dot(chooser, jnp.concatenate(tiles, axis=1).astype(bf16))
            new[0] = jnp.where(inside, placed, old[0].astype(f32)).astype(bf16)


VMEM = pl.BlockSpec(memory_space=pltpu.VMEM)
SMEM = pl.BlockSpec(memory_space=pltpu.SMEM)


def call(body, outs, specs, flops, moved, limit):
    return pl.pallas_call(
        body,
        out_shape=outs,
        in_specs=specs,
        out_specs=jax.tree.map(lambda _: VMEM, outs),
        cost_estimate=pl.CostEstimate(flops=flops, bytes_accessed=moved, transcendentals=0),
        compiler_params=pltpu.CompilerParams(vmem_limit_bytes=limit * MIB),
    )


def shape(*dims, dtype=f32):
    return jax.ShapeDtypeStruct(dims, dtype)


def exchanged(slots, axis):
    return lax.all_to_all(slots, axis, 0, 0, tiled=True)


def shards(
    tokens,
    norm_gain,
    w_query,
    w_key,
    w_value,
    query_gain,
    key_gain,
    head_bias,
    w_output,
    cache_keys,
    cache_values,
    base_length,
    accepted,
    parents,
):
    seqs, prop = parents.shape
    heads = head_bias.shape[0]
    rows, span = seqs * prop, cache_keys.shape[1]
    half = rows // 2
    columns = w_output.shape[1]
    peers = lax.axis_size(KV)
    width = tokens.shape[1] * peers
    assert peers == heads and seqs == 4 and rows <= LANES and heads % 4 == 0 and prop == 16

    sources = (tokens, norm_gain.reshape(1, -1), w_query, w_key, w_value)
    slots = pl.pallas_call(
        project_kernel,
        out_shape=shape(heads, rows + half + 8, LANES),
        in_specs=[pl.BlockSpec(memory_space=pltpu.HBM)] * 5,
        out_specs=VMEM,
        scratch_shapes=[pltpu.VMEM(a.shape, a.dtype) for a in sources] + [pltpu.SemaphoreType.DMA((5,))],
        cost_estimate=pl.CostEstimate(flops=10**8, bytes_accessed=3 * MIB, transcendentals=0),
        compiler_params=pltpu.CompilerParams(vmem_limit_bytes=67_000_000),
    )(*sources)
    got = exchanged(slots, KV)
    slots, own = call(
        functools.partial(normalize_kernel, width),
        (shape(peers, rows + half, LANES, dtype=bf16), shape(rows + half, LANES, dtype=bf16)),
        [VMEM, VMEM, VMEM],
        10**10,
        MIB,
        8,
    )(got, query_gain.reshape(1, -1), key_gain.reshape(1, -1))
    fresh = exchanged(slots, KV)
    slots = call(
        functools.partial(attend_kernel, prop),
        shape(heads, half + prop, LANES),
        [SMEM, SMEM, SMEM, VMEM, VMEM, VMEM],
        4 * 10**8,
        5 * MIB,
        24,
    )(base_length, accepted, head_bias, fresh, cache_keys, cache_values)
    got = exchanged(slots, KV)
    block = pl.BlockSpec((1, span, cache_keys.shape[2]), lambda s: (s, 0, 0))
    tree, updated_keys, updated_values = pl.pallas_call(
        functools.partial(side_kernel, prop),
        grid=(seqs,),
        out_shape=(shape(2, half, LANES), cache_keys, cache_values),
        in_specs=[SMEM, SMEM, SMEM, VMEM, VMEM, VMEM, block, block],
        out_specs=(VMEM, block, block),
        cost_estimate=pl.CostEstimate(flops=10**8, bytes_accessed=8 * MIB, transcendentals=0),
        compiler_params=pltpu.CompilerParams(vmem_limit_bytes=16 * MIB),
    )(base_length, accepted, head_bias, own, parents, fresh, cache_keys, cache_values)
    slots = call(combine_kernel, shape(peers, half, LANES, dtype=bf16), [VMEM] * 2, 10**7, MIB, 8)(got, tree)
    got = exchanged(slots, KV)
    part = call(output_kernel, shape(rows, columns), [VMEM] * 2, 10**8, MIB, 8)(got, w_output)
    other = lax.ppermute(part, "tp", [(0, 1), (1, 0)])
    mix, slots = call(
        squares_kernel, (shape(rows, columns), shape(peers, 8, LANES)), [VMEM] * 2, 10**6, MIB // 4, 4
    )(part, other)
    got = exchanged(slots, KV)
    layer_out = call(
        functools.partial(finish_kernel, columns * peers),
        shape(rows, columns, dtype=bf16),
        [VMEM] * 2,
        10**6,
        MIB // 8,
        4,
    )(mix, got)
    return (layer_out, updated_keys, updated_values)


def solution(mesh):
    finer = Mesh(
        mesh.devices.reshape(mesh.shape["dp"], 4, 4, mesh.shape["tp"]), ("dp", "kv_0", "kv_1", "tp")
    )
    return jax.shard_map(
        shards,
        mesh=finer,
        in_specs=(
            P("dp", KV),
            P(KV),
            P(KV, "tp"),
            P(KV, "tp"),
            P(KV, "tp"),
            P(),
            P(),
            P("tp"),
            P("tp", KV),
            P("dp", KV, "tp"),
            P("dp", KV, "tp"),
            P("dp"),
            P("dp"),
            P("dp", None),
        ),
        out_specs=(P("dp", KV), P("dp", KV, "tp"), P("dp", KV, "tp")),
        check_vma=False,
    )
```

```python
import functools

import jax
import jax.numpy as jnp
from jax import lax
from jax.experimental import pallas as pl
from jax.experimental.pallas import tpu as pltpu
from jax.sharding import Mesh
from jax.sharding import PartitionSpec as P

HEAD_DIM = 64
LANES = 128
KV = ("kv_0", "kv_1")
MIB = 1 << 20
LOG2_E = 1.4426950408889634
HIDDEN = -1e30

epsilon = 1e-05
f32 = jnp.float32
bf16 = jnp.bfloat16


def low_half(rows):
    return lax.broadcasted_iota(jnp.int32, (rows, LANES), 1) < HEAD_DIM


def turned(x):
    return pltpu.roll(x, HEAD_DIM, 1)


def dot(a, b):
    return jnp.dot(a, b, preferred_element_type=f32)


def dot_nt(a, b):
    return lax.dot_general(a, b, (((1,), (1,)), ((), ())), preferred_element_type=f32)


def split_bf16(x, pieces):
    parts = []
    for _ in range(pieces):
        part = x.astype(bf16)
        parts.append(part)
        x = x - part.astype(f32)
    return parts


def signs(z):
    spill = jnp.log(1.0 + jnp.exp(-jnp.abs(z)))
    return -jnp.maximum(z, 0.0) - spill, jnp.minimum(z, 0.0) - spill


def exits(z):
    below, above = jnp.minimum(z, 0.0), jnp.maximum(z, 0.0)
    spill = jnp.log2(1.0 + jnp.exp2(below - above))
    return above + spill, below - spill


def project_kernel(*refs):
    sources, slots, (tokens, gain, w_query, w_key, w_value), arrived = refs[:5], refs[5], refs[6:11], refs[11]
    copies = [
        pltpu.make_async_copy(source, held, arrived.at[at])
        for at, (source, held) in enumerate(zip(sources, refs[6:11]))
    ]
    for copy in copies:
        copy.start()
    rows, half = tokens.shape[0], tokens.shape[0] // 2
    low, low_v = low_half(rows), low_half(half)
    copies[0].wait()
    wide = tokens[...].astype(f32)
    squares = wide * wide
    squares = jnp.concatenate((squares, jnp.zeros((LANES - rows, squares.shape[1]), f32)), axis=0)
    ones = jnp.ones((8, squares.shape[1]), bf16)
    row_squares = sum(dot_nt(ones, part) for part in split_bf16(squares, 3))
    for head in range(slots.shape[0]):
        slots[head, rows + half :] = row_squares
    copies[1].wait()
    scaled = (wide * gain[...]).astype(bf16)
    copies[2].wait()
    copies[3].wait()
    spans = [pl.ds(at, 2 * LANES) for at in range(0, w_query.shape[1], 2 * LANES)]
    tiles = [slice(0, LANES), slice(LANES, 2 * LANES)]
    for at, columns in enumerate(spans):
        query, key = dot(scaled, w_query[:, columns]), dot(scaled, w_key[:, columns])
        for tile, lanes in enumerate(tiles):
            head = 4 * at + 2 * tile
            q, k = query[:, lanes], turned(key[:, lanes])
            slots[head, :rows] = jnp.where(low, q, k)
            slots[head + 1, :rows] = jnp.where(low, k, q)
    copies[4].wait()
    for at, columns in enumerate(spans):
        value = dot(scaled, w_value[:, columns])
        for tile, lanes in enumerate(tiles):
            head = 4 * at + 2 * tile
            v = value[:, lanes]
            v_turned = turned(v)
            slots[head, rows : rows + half] = jnp.where(low_v, v[:half], v_turned[half:])
            slots[head + 1, rows : rows + half] = jnp.where(low_v, v_turned[:half], v[half:])


def normalize_kernel(width, got, query_gain, key_gain, slots, own):
    peers = got.shape[0]
    rows = got.shape[1] - 8
    half = rows // 3
    rows = 2 * half
    even = lax.axis_index(KV) % 2 == 0
    total = got[0]
    for peer in range(1, peers):
        total = total + got[peer]
    both, value, squares = total[:rows], total[rows : rows + half], total[rows + half : rows + half + 1]
    low = low_half(rows)
    power = both * both
    low_sum = jnp.sum(jnp.where(low, power, 0.0), axis=1, keepdims=True)
    high_sum = jnp.sum(jnp.where(low, 0.0, power), axis=1, keepdims=True)
    factor = lax.rsqrt(jnp.where(low, low_sum, high_sum) / HEAD_DIM + epsilon)
    one, two = query_gain[...], key_gain[...]
    gain = jnp.concatenate((jnp.where(even, one, two), jnp.where(even, two, one)), axis=1)
    normed = (both * factor * gain).astype(bf16)
    inv_rms = jnp.broadcast_to(lax.rsqrt(squares / width + epsilon), (half, LANES))
    lane = lax.broadcasted_iota(jnp.int32, (half, LANES), 1)
    row = lax.broadcasted_iota(jnp.int32, (half, LANES), 0)
    first = jnp.sum(jnp.where(lane == row, inv_rms, 0.0), axis=1, keepdims=True)
    second = jnp.sum(jnp.where(lane == row + half, inv_rms, 0.0), axis=1, keepdims=True)
    fresh = (value * jnp.where(lane < HEAD_DIM, first, second)).astype(bf16)
    own[:rows] = normed
    own[rows:] = fresh
    for peer in range(peers):
        slots[peer, :rows] = normed
        slots[peer, rows:] = fresh


def tree_part(prop, bias, own, parents, out):
    half = own.shape[0] // 3
    rows = 2 * half
    even = lax.axis_index(KV) % 2 == 0
    low = low_half(rows)
    both = own[:rows].astype(f32)
    other = turned(both)
    query = jnp.where(low, jnp.where(even, both, other), 0.0).astype(bf16)
    key = jnp.where(even, other, both).astype(bf16)
    score = dot_nt(query, key) * HEAD_DIM ** (-0.5) + bias[lax.axis_index(KV)]
    row = lax.broadcasted_iota(jnp.int32, (rows, rows), 0)
    column = lax.broadcasted_iota(jnp.int32, (rows, rows), 1)
    small = [lax.broadcasted_iota(jnp.int32, (prop, prop), axis) for axis in range(2)]
    parent = jnp.concatenate(
        [
            jnp.sum(jnp.where(small[0] == small[1], parents[seq : seq + 1], 0), axis=1, keepdims=True)
            for seq in range(rows // prop)
        ],
        axis=0,
    )
    direct = (parent >= 0) & (column == row - row % prop + parent)
    step = jnp.where(direct, 1.0, 0.0).astype(bf16)
    above = jnp.where(row == column, 1.0, 0.0)
    above = above + step.astype(f32)
    reach = 2
    while reach < prop:
        step = dot(step, step).astype(bf16)
        above = above + dot(above.astype(bf16), step)
        reach *= 2
    mine = (above > 0.5) & (row != column)
    stay, taken = signs(score)
    stay = jnp.where(mine, stay, 0.0)
    after = jnp.where(row > column, 1.0, 0.0).astype(bf16)
    tail = sum(dot(part, after) for part in split_bf16(stay, 3))
    weight = jnp.where(mine, jnp.exp(taken + tail), 0.0).astype(bf16)
    kept = jnp.exp(jnp.sum(stay, axis=1, keepdims=True))
    value = own[rows:].astype(f32)
    value = jnp.concatenate((value, turned(value)), axis=0).astype(bf16)
    summed = dot(weight, value)
    low = low_half(half)
    out[0] = jnp.where(low, summed[:half], turned(summed[half:]))
    out[1] = jnp.where(low, kept[:half], kept[half:])


def attend_kernel(prop, base, accepted, bias, fresh, keys, values, slots, held, sent):
    seqs, span, _ = keys.shape
    heads = fresh.shape[0]
    half = seqs * prop // 2
    group = 4
    groups = heads // group
    low = low_half(prop)
    low_mask = low.astype(f32).astype(bf16)
    high_mask = (1.0 - low.astype(f32)).astype(bf16)
    blank = jnp.zeros((prop, LANES), bf16)
    order = lax.broadcasted_iota(jnp.int32, (span, span), 0)
    after = jnp.where(order > lax.broadcasted_iota(jnp.int32, (span, span), 1), 1.0, 0.0).astype(bf16)
    position = lax.axis_index(KV) * span + lax.broadcasted_iota(jnp.int32, (1, span), 1)
    hidden = [jnp.where(position < base[seq] + accepted[seq], 0.0, HIDDEN) for seq in range(seqs)]
    quarter = lax.broadcasted_iota(jnp.int32, (prop, LANES), 1) // (LANES // seqs)
    sending = []

    def scored(at):
        first, scores = at * group, []
        for seq in range(seqs):
            blocks = []
            for j in range(group):
                tile = fresh[first + j, seq * prop : (seq + 1) * prop] * (low_mask if j % 2 == 0 else high_mask)
                blocks.append(jnp.concatenate((tile, blank) if j < 2 else (blank, tile), axis=1))
            stored = keys[seq, :, first * HEAD_DIM : (first + group) * HEAD_DIM]
            score = dot_nt(jnp.concatenate(blocks, axis=0), stored)
            for j in range(group):
                part = score[j * prop : (j + 1) * prop]
                scores.append(part * (HEAD_DIM ** (-0.5) * LOG2_E) + (bias[first + j] * LOG2_E + hidden[seq]))
        return jnp.concatenate(scores, axis=0)

    def suffixes(score):
        leave, taken = exits(score)
        tall = leave.shape[0]
        tail = dot(jnp.concatenate(split_bf16(leave, 2), axis=0), after)
        tail = tail[:tall] + tail[tall:]
        log = tail[:, :1] + leave[:, :1]
        return jnp.exp2(taken - tail).astype(bf16), log

    def send(at, weight, log):
        first, tiles = at * group, []
        for seq in range(seqs):
            stored = values[seq, :, first * HEAD_DIM : (first + group) * HEAD_DIM]
            tiles.append(dot(weight[seq * group * prop : (seq + 1) * group * prop], stored))
        for j in range(group):
            head = first + j
            rows = slice(j * prop, (j + 1) * prop)
            lanes = slice(j // 2 * LANES, (j // 2 + 1) * LANES)
            for seq in range(seqs // 2):
                one, two = tiles[seq][rows, lanes], tiles[seq + seqs // 2][rows, lanes]
                one, two = (one, turned(two)) if j % 2 == 0 else (turned(one), two)
                held[head, seq * prop : (seq + 1) * prop] = jnp.where(low, one, two)
            logs = jnp.zeros((prop, LANES), f32)
            for seq in range(seqs):
                start = (seq * group + j) * prop
                logs = jnp.where(quarter == seq, log[start : start + prop], logs)
            held[head, half:] = logs
        chosen = pl.ds(first, group)
        copy = pltpu.make_async_copy(held.at[chosen], slots.at[chosen], sent.at[at])
        copy.start()
        sending.append(copy)

    score, ready = scored(0), None
    for at in range(groups):
        following = scored(at + 1) if at + 1 < groups else None
        weight, log = suffixes(score)
        if ready is not None:
            send(at - 1, *ready)
        ready, score = (weight, log), following
    send(groups - 1, *ready)
    for copy in sending:
        copy.wait()


def combine_kernel(got, tree, slots):
    blocks, tall, _ = got.shape
    prop = tall // 3
    half = 2 * prop
    lane = lax.broadcasted_iota(jnp.int32, (prop, LANES), 1)
    first = lane % HEAD_DIM < HEAD_DIM // 2
    later = jnp.zeros((prop, LANES), f32)
    part = jnp.zeros((half, LANES), f32)
    for block in range(blocks - 1, -1, -1):
        kept = jnp.exp2(-later)
        one = jnp.where(first, kept, pltpu.roll(kept, HEAD_DIM // 2, 1))
        two = jnp.where(first, pltpu.roll(kept, LANES - HEAD_DIM // 2, 1), kept)
        part = part + jnp.concatenate((one, two), axis=0) * got[block, :half]
        later = later + got[block, half:]
    attended = (tree[0] + tree[1] * part).astype(bf16)
    for block in range(blocks):
        slots[block] = attended


def output_kernel(got, w_output, out):
    heads, half, _ = got.shape
    low = low_half(half)
    columns = []
    for head in range(0, heads, 2):
        one, two = got[head].astype(f32), got[head + 1].astype(f32)
        top = jnp.where(low, one, turned(two))
        bottom = jnp.where(low, turned(one), two)
        columns.append(jnp.concatenate((top, bottom), axis=0).astype(bf16))
    out[...] = dot(jnp.concatenate(columns, axis=1), w_output[...])


def squares_kernel(one, two, mix, slots):
    total = one[...] + two[...]
    mix[...] = total
    rows = total.shape[0]
    squares = jnp.sum(total * total, axis=1, keepdims=True)
    lane = lax.broadcasted_iota(jnp.int32, (rows, LANES), 1)
    row = lax.broadcasted_iota(jnp.int32, (rows, LANES), 0)
    flat = jnp.sum(jnp.where(lane == row, squares, 0.0), axis=0, keepdims=True)
    slots[...] = jnp.broadcast_to(flat[None], slots.shape)


def finish_kernel(width, mix, got, out):
    total = got[0]
    for peer in range(1, got.shape[0]):
        total = total + got[peer]
    rows = out.shape[0]
    factor = jnp.broadcast_to(lax.rsqrt(total[:1] / width + epsilon), (rows, LANES))
    lane = lax.broadcasted_iota(jnp.int32, (rows, LANES), 1)
    row = lax.broadcasted_iota(jnp.int32, (rows, LANES), 0)
    factor = jnp.sum(jnp.where(lane == row, factor, 0.0), axis=1, keepdims=True)
    out[...] = (mix[...] * factor).astype(bf16)


def side_kernel(
    prop, base, accepted, bias, own, parents, fresh, keys, values, tree, new_keys, new_values, held, moved
):
    seqs, span, _ = keys.shape
    heads = fresh.shape[0]
    rows = seqs * prop
    window = 2 * prop
    loads, stores = [], []
    for seq in range(seqs):
        for which, (source, target) in enumerate(((keys, new_keys), (values, new_values))):
            block = held.at[which, seq]
            loads.append(pltpu.make_async_copy(source.at[seq], block, moved.at[0, which, seq]))
            stores.append(pltpu.make_async_copy(block, target.at[seq], moved.at[1, which, seq]))
    for copy in loads:
        copy.start()
    tree_part(prop, bias, own, parents, tree)
    low = low_half(prop)
    for seq in range(seqs):
        start = base[seq] + accepted[seq] - lax.axis_index(KV) * span
        at = jnp.minimum(jnp.maximum(start, 0), span - window) // prop * prop
        lines = pl.ds(pl.multiple_of(at, prop), window)
        start = start - at
        early = seq < seqs // 2
        key_rows = slice(seq * prop, (seq + 1) * prop)
        value_rows = slice(rows + seq % (seqs // 2) * prop, rows + (seq % (seqs // 2) + 1) * prop)
        key_tiles, value_tiles = [], []
        for head in range(0, heads, 2):
            one, two = fresh[head, key_rows].astype(f32), fresh[head + 1, key_rows].astype(f32)
            key_tiles.append(turned(jnp.where(low, two, one)))
            one, two = fresh[head, value_rows].astype(f32), fresh[head + 1, value_rows].astype(f32)
            value_tiles.append(jnp.where(low, one, turned(two)) if early else jnp.where(low, turned(one), two))
        offset = lax.broadcasted_iota(jnp.int32, (window, prop), 0) - start
        chooser = jnp.where(offset == lax.broadcasted_iota(jnp.int32, (window, prop), 1), 1.0, 0.0).astype(bf16)
        offset = lax.broadcasted_iota(jnp.int32, (window, 1), 0) - start
        inside = (offset >= 0) & (offset < prop)
        for which, tiles in enumerate((key_tiles, value_tiles)):
            placed = dot(chooser, jnp.concatenate(tiles, axis=1).astype(bf16))
            loads[2 * seq + which].wait()
            old = held[which, seq, lines].astype(f32)
            held[which, seq, lines] = jnp.where(inside, placed, old).astype(bf16)
            stores[2 * seq + which].start()
    for copy in stores:
        copy.wait()


VMEM = pl.BlockSpec(memory_space=pltpu.VMEM)
SMEM = pl.BlockSpec(memory_space=pltpu.SMEM)


def call(body, outs, specs, flops, moved, limit):
    return pl.pallas_call(
        body,
        out_shape=outs,
        in_specs=specs,
        out_specs=jax.tree.map(lambda _: VMEM, outs),
        cost_estimate=pl.CostEstimate(flops=flops, bytes_accessed=moved, transcendentals=0),
        compiler_params=pltpu.CompilerParams(vmem_limit_bytes=limit * MIB),
    )


def shape(*dims, dtype=f32):
    return jax.ShapeDtypeStruct(dims, dtype)


def exchanged(slots, axis):
    return lax.all_to_all(slots, axis, 0, 0, tiled=True)


def shards(
    tokens,
    norm_gain,
    w_query,
    w_key,
    w_value,
    query_gain,
    key_gain,
    head_bias,
    w_output,
    cache_keys,
    cache_values,
    base_length,
    accepted,
    parents,
):
    seqs, prop = parents.shape
    heads = head_bias.shape[0]
    rows, span = seqs * prop, cache_keys.shape[1]
    half = rows // 2
    columns = w_output.shape[1]
    peers = lax.axis_size(KV)
    width = tokens.shape[1] * peers
    assert peers == heads and seqs == 4 and rows <= LANES and heads % 4 == 0 and prop == 16

    hbm = pl.BlockSpec(memory_space=pltpu.HBM)
    sources = [
        pltpu.with_memory_space_constraint(a, pltpu.HBM)
        for a in (tokens, norm_gain.reshape(1, -1), w_query, w_key, w_value)
    ]
    slots = pl.pallas_call(
        project_kernel,
        out_shape=pltpu.VMEM((heads, rows + half + 8, LANES), f32),
        in_specs=[hbm] * 5,
        out_specs=VMEM,
        scratch_shapes=[pltpu.VMEM(a.shape, a.dtype) for a in sources] + [pltpu.SemaphoreType.DMA((5,))],
        cost_estimate=pl.CostEstimate(flops=10**8, bytes_accessed=3 * MIB, transcendentals=0),
        compiler_params=pltpu.CompilerParams(vmem_limit_bytes=12 * MIB),
    )(*sources)
    got = exchanged(slots, KV)
    slots, own = call(
        functools.partial(normalize_kernel, width),
        (shape(peers, rows + half, LANES, dtype=bf16), shape(rows + half, LANES, dtype=bf16)),
        [VMEM, VMEM, VMEM],
        10**10,
        MIB,
        8,
    )(got, query_gain.reshape(1, -1), key_gain.reshape(1, -1))
    fresh = exchanged(slots, KV)
    slots = pl.pallas_call(
        functools.partial(attend_kernel, prop),
        out_shape=shape(heads, half + prop, LANES),
        in_specs=[SMEM, SMEM, SMEM, VMEM, VMEM, VMEM],
        out_specs=hbm,
        scratch_shapes=[pltpu.VMEM((heads, half + prop, LANES), f32), pltpu.SemaphoreType.DMA((heads // 4,))],
        cost_estimate=pl.CostEstimate(flops=4 * 10**8, bytes_accessed=5 * MIB, transcendentals=0),
        compiler_params=pltpu.CompilerParams(vmem_limit_bytes=24 * MIB),
    )(base_length, accepted, head_bias, fresh, cache_keys, cache_values)
    got = exchanged(slots, KV)
    stored = [pltpu.with_memory_space_constraint(a, pltpu.HBM) for a in (cache_keys, cache_values)]
    tree, updated_keys, updated_values = pl.pallas_call(
        functools.partial(side_kernel, prop),
        out_shape=(shape(2, half, LANES), cache_keys, cache_values),
        in_specs=[SMEM, SMEM, SMEM, VMEM, VMEM, VMEM, hbm, hbm],
        out_specs=(VMEM, hbm, hbm),
        scratch_shapes=[pltpu.VMEM((2, *cache_keys.shape), bf16), pltpu.SemaphoreType.DMA((2, 2, seqs))],
        cost_estimate=pl.CostEstimate(flops=10**8, bytes_accessed=8 * MIB, transcendentals=0),
        compiler_params=pltpu.CompilerParams(vmem_limit_bytes=16 * MIB),
    )(base_length, accepted, head_bias, own, parents, fresh, *stored)
    slots = call(combine_kernel, shape(peers, half, LANES, dtype=bf16), [VMEM] * 2, 10**7, MIB, 8)(got, tree)
    got = exchanged(slots, KV)
    part = call(output_kernel, shape(rows, columns), [VMEM] * 2, 10**8, MIB, 8)(got, w_output)
    other = lax.ppermute(part, "tp", [(0, 1), (1, 0)])
    mix, slots = call(
        squares_kernel, (shape(rows, columns), shape(peers, 8, LANES)), [VMEM] * 2, 10**6, MIB // 4, 4
    )(part, other)
    got = exchanged(slots, KV)
    layer_out = call(
        functools.partial(finish_kernel, columns * peers),
        shape(rows, columns, dtype=bf16),
        [VMEM] * 2,
        10**6,
        MIB // 8,
        4,
    )(mix, got)
    return (layer_out, updated_keys, updated_values)


def solution(mesh):
    finer = Mesh(
        mesh.devices.reshape(mesh.shape["dp"], 4, 4, mesh.shape["tp"]), ("dp", "kv_0", "kv_1", "tp")
    )
    return jax.shard_map(
        shards,
        mesh=finer,
        in_specs=(
            P("dp", KV),
            P(KV),
            P(KV, "tp"),
            P(KV, "tp"),
            P(KV, "tp"),
            P(),
            P(),
            P("tp"),
            P("tp", KV),
            P("dp", KV, "tp"),
            P("dp", KV, "tp"),
            P("dp"),
            P("dp"),
            P("dp", None),
        ),
        out_specs=(P("dp", KV), P("dp", KV, "tp"), P("dp", KV, "tp")),
        check_vma=False,
    )
```

```python
import functools

import jax
import jax.numpy as jnp
from jax import lax
from jax.experimental import pallas as pl
from jax.experimental.pallas import tpu as pltpu
from jax.sharding import Mesh
from jax.sharding import PartitionSpec as P

HEAD_DIM = 64
LANES = 128
KV = ("kv_0", "kv_1")
MIB = 1 << 20
LOG2_E = 1.4426950408889634
HIDDEN = -1e30

epsilon = 1e-05
f32 = jnp.float32
bf16 = jnp.bfloat16


def low_half(rows):
    return lax.broadcasted_iota(jnp.int32, (rows, LANES), 1) < HEAD_DIM


def turned(x):
    return pltpu.roll(x, HEAD_DIM, 1)


def dot(a, b):
    return jnp.dot(a, b, preferred_element_type=f32)


def dot_nt(a, b):
    return lax.dot_general(a, b, (((1,), (1,)), ((), ())), preferred_element_type=f32)


def split_bf16(x, pieces):
    parts = []
    for _ in range(pieces):
        part = x.astype(bf16)
        parts.append(part)
        x = x - part.astype(f32)
    return parts


def signs(z):
    spill = jnp.log(1.0 + jnp.exp(-jnp.abs(z)))
    return -jnp.maximum(z, 0.0) - spill, jnp.minimum(z, 0.0) - spill


def exits(z):
    below, above = jnp.minimum(z, 0.0), jnp.maximum(z, 0.0)
    spill = jnp.log2(1.0 + jnp.exp2(below - above))
    return above + spill, below - spill


def project_kernel(*refs):
    sources, slots, (tokens, gain, w_query, w_key, w_value), arrived = refs[:5], refs[5], refs[6:11], refs[11]
    copies = [
        pltpu.make_async_copy(source, held, arrived.at[at])
        for at, (source, held) in enumerate(zip(sources, refs[6:11]))
    ]
    for copy in copies:
        copy.start()
    rows, half = tokens.shape[0], tokens.shape[0] // 2
    low, low_v = low_half(rows), low_half(half)
    copies[0].wait()
    wide = tokens[...].astype(f32)
    squares = wide * wide
    squares = jnp.concatenate((squares, jnp.zeros((LANES - rows, squares.shape[1]), f32)), axis=0)
    ones = jnp.ones((8, squares.shape[1]), bf16)
    row_squares = sum(dot_nt(ones, part) for part in split_bf16(squares, 3))
    for head in range(slots.shape[0]):
        slots[head, rows + half :] = row_squares
    copies[1].wait()
    scaled = (wide * gain[...]).astype(bf16)
    copies[2].wait()
    copies[3].wait()
    spans = [pl.ds(at, 2 * LANES) for at in range(0, w_query.shape[1], 2 * LANES)]
    tiles = [slice(0, LANES), slice(LANES, 2 * LANES)]
    for at, columns in enumerate(spans):
        query, key = dot(scaled, w_query[:, columns]), dot(scaled, w_key[:, columns])
        for tile, lanes in enumerate(tiles):
            head = 4 * at + 2 * tile
            q, k = query[:, lanes], turned(key[:, lanes])
            slots[head, :rows] = jnp.where(low, q, k)
            slots[head + 1, :rows] = jnp.where(low, k, q)
    copies[4].wait()
    for at, columns in enumerate(spans):
        value = dot(scaled, w_value[:, columns])
        for tile, lanes in enumerate(tiles):
            head = 4 * at + 2 * tile
            v = value[:, lanes]
            v_turned = turned(v)
            slots[head, rows : rows + half] = jnp.where(low_v, v[:half], v_turned[half:])
            slots[head + 1, rows : rows + half] = jnp.where(low_v, v_turned[:half], v[half:])


def normalize_kernel(width, got, query_gain, key_gain, slots, own):
    peers = got.shape[0]
    rows = got.shape[1] - 8
    half = rows // 3
    rows = 2 * half
    even = lax.axis_index(KV) % 2 == 0
    total = got[0]
    for peer in range(1, peers):
        total = total + got[peer]
    both, value, squares = total[:rows], total[rows : rows + half], total[rows + half : rows + half + 1]
    low = low_half(rows)
    power = both * both
    low_sum = jnp.sum(jnp.where(low, power, 0.0), axis=1, keepdims=True)
    high_sum = jnp.sum(jnp.where(low, 0.0, power), axis=1, keepdims=True)
    factor = lax.rsqrt(jnp.where(low, low_sum, high_sum) / HEAD_DIM + epsilon)
    one, two = query_gain[...], key_gain[...]
    gain = jnp.concatenate((jnp.where(even, one, two), jnp.where(even, two, one)), axis=1)
    normed = (both * factor * gain).astype(bf16)
    inv_rms = jnp.broadcast_to(lax.rsqrt(squares / width + epsilon), (half, LANES))
    lane = lax.broadcasted_iota(jnp.int32, (half, LANES), 1)
    row = lax.broadcasted_iota(jnp.int32, (half, LANES), 0)
    first = jnp.sum(jnp.where(lane == row, inv_rms, 0.0), axis=1, keepdims=True)
    second = jnp.sum(jnp.where(lane == row + half, inv_rms, 0.0), axis=1, keepdims=True)
    fresh = (value * jnp.where(lane < HEAD_DIM, first, second)).astype(bf16)
    own[:rows] = normed
    own[rows:] = fresh
    for peer in range(peers):
        slots[peer, :rows] = normed
        slots[peer, rows:] = fresh


def tree_part(prop, bias, own, parents, out):
    half = own.shape[0] // 3
    rows = 2 * half
    even = lax.axis_index(KV) % 2 == 0
    low = low_half(rows)
    both = own[:rows].astype(f32)
    other = turned(both)
    query = jnp.where(low, jnp.where(even, both, other), 0.0).astype(bf16)
    key = jnp.where(even, other, both).astype(bf16)
    score = dot_nt(query, key) * HEAD_DIM ** (-0.5) + bias[lax.axis_index(KV)]
    row = lax.broadcasted_iota(jnp.int32, (rows, rows), 0)
    column = lax.broadcasted_iota(jnp.int32, (rows, rows), 1)
    small = [lax.broadcasted_iota(jnp.int32, (prop, prop), axis) for axis in range(2)]
    parent = jnp.concatenate(
        [
            jnp.sum(jnp.where(small[0] == small[1], parents[seq : seq + 1], 0), axis=1, keepdims=True)
            for seq in range(rows // prop)
        ],
        axis=0,
    )
    direct = (parent >= 0) & (column == row - row % prop + parent)
    step = jnp.where(direct, 1.0, 0.0).astype(bf16)
    above = jnp.where(row == column, 1.0, 0.0)
    above = above + step.astype(f32)
    reach = 2
    while reach < prop:
        step = dot(step, step).astype(bf16)
        above = above + dot(above.astype(bf16), step)
        reach *= 2
    mine = (above > 0.5) & (row != column)
    stay, taken = signs(score)
    stay = jnp.where(mine, stay, 0.0)
    after = jnp.where(row > column, 1.0, 0.0).astype(bf16)
    tail = sum(dot(part, after) for part in split_bf16(stay, 3))
    weight = jnp.where(mine, jnp.exp(taken + tail), 0.0).astype(bf16)
    kept = jnp.exp(jnp.sum(stay, axis=1, keepdims=True))
    value = own[rows:].astype(f32)
    value = jnp.concatenate((value, turned(value)), axis=0).astype(bf16)
    summed = dot(weight, value)
    low = low_half(half)
    out[0] = jnp.where(low, summed[:half], turned(summed[half:]))
    out[1] = jnp.where(low, kept[:half], kept[half:])


def attend_kernel(prop, base, accepted, bias, fresh, keys, values, slots, held, sent):
    seqs, span, _ = keys.shape
    heads = fresh.shape[0]
    half = seqs * prop // 2
    group = 4
    groups = heads // group
    low = low_half(prop)
    low_mask = low.astype(f32).astype(bf16)
    high_mask = (1.0 - low.astype(f32)).astype(bf16)
    blank = jnp.zeros((prop, LANES), bf16)
    order = lax.broadcasted_iota(jnp.int32, (span, span), 0)
    after = jnp.where(order > lax.broadcasted_iota(jnp.int32, (span, span), 1), 1.0, 0.0).astype(bf16)
    position = lax.axis_index(KV) * span + lax.broadcasted_iota(jnp.int32, (1, span), 1)
    valid = base[...] + accepted[...]
    hidden = [jnp.where(position < valid[:, seq : seq + 1], 0.0, HIDDEN) for seq in range(seqs)]
    offset = bias[...] * LOG2_E
    quarter = lax.broadcasted_iota(jnp.int32, (prop, LANES), 1) // (LANES // seqs)
    sending = []

    def scored(at):
        first, scores = at * group, []
        for seq in range(seqs):
            blocks = []
            for j in range(group):
                tile = fresh[first + j, seq * prop : (seq + 1) * prop] * (low_mask if j % 2 == 0 else high_mask)
                blocks.append(jnp.concatenate((tile, blank) if j < 2 else (blank, tile), axis=1))
            stored = keys[seq, :, first * HEAD_DIM : (first + group) * HEAD_DIM]
            score = dot_nt(jnp.concatenate(blocks, axis=0), stored)
            for j in range(group):
                part = score[j * prop : (j + 1) * prop]
                scores.append(part * (HEAD_DIM ** (-0.5) * LOG2_E) + (offset[:, first + j : first + j + 1] + hidden[seq]))
        return jnp.concatenate(scores, axis=0)

    def suffixes(score):
        leave, taken = exits(score)
        tall = leave.shape[0]
        tail = dot(jnp.concatenate(split_bf16(leave, 2), axis=0), after)
        tail = tail[:tall] + tail[tall:]
        log = tail[:, :1] + leave[:, :1]
        return jnp.exp2(taken - tail).astype(bf16), log

    def send(at, weight, log):
        first, tiles = at * group, []
        for seq in range(seqs):
            stored = values[seq, :, first * HEAD_DIM : (first + group) * HEAD_DIM]
            tiles.append(dot(weight[seq * group * prop : (seq + 1) * group * prop], stored))
        for j in range(group):
            head = first + j
            rows = slice(j * prop, (j + 1) * prop)
            lanes = slice(j // 2 * LANES, (j // 2 + 1) * LANES)
            for seq in range(seqs // 2):
                one, two = tiles[seq][rows, lanes], tiles[seq + seqs // 2][rows, lanes]
                one, two = (one, turned(two)) if j % 2 == 0 else (turned(one), two)
                held[head, seq * prop : (seq + 1) * prop] = jnp.where(low, one, two)
            logs = jnp.zeros((prop, LANES), f32)
            for seq in range(seqs):
                start = (seq * group + j) * prop
                logs = jnp.where(quarter == seq, log[start : start + prop], logs)
            held[head, half:] = logs
        chosen = pl.ds(first, group)
        copy = pltpu.make_async_copy(held.at[chosen], slots.at[chosen], sent.at[at])
        copy.start()
        sending.append(copy)

    score, ready = scored(0), None
    for at in range(groups):
        following = scored(at + 1) if at + 1 < groups else None
        weight, log = suffixes(score)
        if ready is not None:
            send(at - 1, *ready)
        ready, score = (weight, log), following
    send(groups - 1, *ready)
    for copy in sending:
        copy.wait()


def combine_kernel(got, tree, slots):
    blocks, tall, _ = got.shape
    prop = tall // 3
    half = 2 * prop
    lane = lax.broadcasted_iota(jnp.int32, (prop, LANES), 1)
    first = lane % HEAD_DIM < HEAD_DIM // 2
    later = jnp.zeros((prop, LANES), f32)
    part = jnp.zeros((half, LANES), f32)
    for block in range(blocks - 1, -1, -1):
        kept = jnp.exp2(-later)
        one = jnp.where(first, kept, pltpu.roll(kept, HEAD_DIM // 2, 1))
        two = jnp.where(first, pltpu.roll(kept, LANES - HEAD_DIM // 2, 1), kept)
        part = part + jnp.concatenate((one, two), axis=0) * got[block, :half]
        later = later + got[block, half:]
    attended = (tree[0] + tree[1] * part).astype(bf16)
    for block in range(blocks):
        slots[block] = attended


def output_kernel(got, w_output, out):
    heads, half, _ = got.shape
    low = low_half(half)
    columns = []
    for head in range(0, heads, 2):
        one, two = got[head].astype(f32), got[head + 1].astype(f32)
        top = jnp.where(low, one, turned(two))
        bottom = jnp.where(low, turned(one), two)
        columns.append(jnp.concatenate((top, bottom), axis=0).astype(bf16))
    out[...] = dot(jnp.concatenate(columns, axis=1), w_output[...])


def squares_kernel(one, two, mix, slots):
    total = one[...] + two[...]
    mix[...] = total
    rows = total.shape[0]
    squares = jnp.sum(total * total, axis=1, keepdims=True)
    lane = lax.broadcasted_iota(jnp.int32, (rows, LANES), 1)
    row = lax.broadcasted_iota(jnp.int32, (rows, LANES), 0)
    flat = jnp.sum(jnp.where(lane == row, squares, 0.0), axis=0, keepdims=True)
    slots[...] = jnp.broadcast_to(flat[None], slots.shape)


def finish_kernel(width, mix, got, out):
    total = got[0]
    for peer in range(1, got.shape[0]):
        total = total + got[peer]
    rows = out.shape[0]
    factor = jnp.broadcast_to(lax.rsqrt(total[:1] / width + epsilon), (rows, LANES))
    lane = lax.broadcasted_iota(jnp.int32, (rows, LANES), 1)
    row = lax.broadcasted_iota(jnp.int32, (rows, LANES), 0)
    factor = jnp.sum(jnp.where(lane == row, factor, 0.0), axis=1, keepdims=True)
    out[...] = (mix[...] * factor).astype(bf16)


def side_kernel(
    prop, base, accepted, bias, own, parents, fresh, keys, values, tree, new_keys, new_values, held, moved
):
    seqs, span, _ = keys.shape
    heads = fresh.shape[0]
    rows = seqs * prop
    window = 2 * prop
    loads, stores = [], []
    for seq in range(seqs):
        for which, (source, target) in enumerate(((keys, new_keys), (values, new_values))):
            block = held.at[which, seq]
            loads.append(pltpu.make_async_copy(source.at[seq], block, moved.at[0, which, seq]))
            stores.append(pltpu.make_async_copy(block, target.at[seq], moved.at[1, which, seq]))
    for copy in loads:
        copy.start()
    tree_part(prop, bias, own, parents, tree)
    low = low_half(prop)
    for seq in range(seqs):
        start = base[seq] + accepted[seq] - lax.axis_index(KV) * span
        at = jnp.minimum(jnp.maximum(start, 0), span - window) // prop * prop
        lines = pl.ds(pl.multiple_of(at, prop), window)
        start = start - at
        early = seq < seqs // 2
        key_rows = slice(seq * prop, (seq + 1) * prop)
        value_rows = slice(rows + seq % (seqs // 2) * prop, rows + (seq % (seqs // 2) + 1) * prop)
        key_tiles, value_tiles = [], []
        for head in range(0, heads, 2):
            one, two = fresh[head, key_rows].astype(f32), fresh[head + 1, key_rows].astype(f32)
            key_tiles.append(turned(jnp.where(low, two, one)))
            one, two = fresh[head, value_rows].astype(f32), fresh[head + 1, value_rows].astype(f32)
            value_tiles.append(jnp.where(low, one, turned(two)) if early else jnp.where(low, turned(one), two))
        offset = lax.broadcasted_iota(jnp.int32, (window, prop), 0) - start
        chooser = jnp.where(offset == lax.broadcasted_iota(jnp.int32, (window, prop), 1), 1.0, 0.0).astype(bf16)
        offset = lax.broadcasted_iota(jnp.int32, (window, 1), 0) - start
        inside = (offset >= 0) & (offset < prop)
        for which, tiles in enumerate((key_tiles, value_tiles)):
            placed = dot(chooser, jnp.concatenate(tiles, axis=1).astype(bf16))
            loads[2 * seq + which].wait()
            old = held[which, seq, lines].astype(f32)
            held[which, seq, lines] = jnp.where(inside, placed, old).astype(bf16)
            stores[2 * seq + which].start()
    for copy in stores:
        copy.wait()


VMEM = pl.BlockSpec(memory_space=pltpu.VMEM)
SMEM = pl.BlockSpec(memory_space=pltpu.SMEM)


def call(body, outs, specs, flops, moved, limit):
    return pl.pallas_call(
        body,
        out_shape=outs,
        in_specs=specs,
        out_specs=jax.tree.map(lambda _: VMEM, outs),
        cost_estimate=pl.CostEstimate(flops=flops, bytes_accessed=moved, transcendentals=0),
        compiler_params=pltpu.CompilerParams(vmem_limit_bytes=limit * MIB),
    )


def shape(*dims, dtype=f32):
    return jax.ShapeDtypeStruct(dims, dtype)


def exchanged(slots, axis):
    return lax.all_to_all(slots, axis, 0, 0, tiled=True)


def shards(
    tokens,
    norm_gain,
    w_query,
    w_key,
    w_value,
    query_gain,
    key_gain,
    head_bias,
    w_output,
    cache_keys,
    cache_values,
    base_length,
    accepted,
    parents,
):
    seqs, prop = parents.shape
    heads = head_bias.shape[0]
    rows, span = seqs * prop, cache_keys.shape[1]
    half = rows // 2
    columns = w_output.shape[1]
    peers = lax.axis_size(KV)
    width = tokens.shape[1] * peers
    assert peers == heads and seqs == 4 and rows <= LANES and heads % 4 == 0 and prop == 16

    hbm = pl.BlockSpec(memory_space=pltpu.HBM)
    sources = [
        pltpu.with_memory_space_constraint(a, pltpu.HBM)
        for a in (tokens, norm_gain.reshape(1, -1), w_query, w_key, w_value)
    ]
    slots = pl.pallas_call(
        project_kernel,
        out_shape=pltpu.VMEM((heads, rows + half + 8, LANES), f32),
        in_specs=[hbm] * 5,
        out_specs=VMEM,
        scratch_shapes=[pltpu.VMEM(a.shape, a.dtype) for a in sources] + [pltpu.SemaphoreType.DMA((5,))],
        cost_estimate=pl.CostEstimate(flops=10**8, bytes_accessed=3 * MIB, transcendentals=0),
        compiler_params=pltpu.CompilerParams(vmem_limit_bytes=12 * MIB),
    )(*sources)
    got = exchanged(slots, KV)
    slots, own = call(
        functools.partial(normalize_kernel, width),
        (shape(peers, rows + half, LANES, dtype=bf16), shape(rows + half, LANES, dtype=bf16)),
        [VMEM, VMEM, VMEM],
        10**10,
        MIB,
        8,
    )(got, query_gain.reshape(1, -1), key_gain.reshape(1, -1))
    fresh = exchanged(slots, KV)
    slots = pl.pallas_call(
        functools.partial(attend_kernel, prop),
        out_shape=shape(heads, half + prop, LANES),
        in_specs=[VMEM] * 6,
        out_specs=hbm,
        scratch_shapes=[pltpu.VMEM((heads, half + prop, LANES), f32), pltpu.SemaphoreType.DMA((heads // 4,))],
        cost_estimate=pl.CostEstimate(flops=4 * 10**8, bytes_accessed=5 * MIB, transcendentals=0),
        compiler_params=pltpu.CompilerParams(vmem_limit_bytes=24 * MIB),
    )(*(a.reshape(1, -1) for a in (base_length, accepted, head_bias)), fresh, cache_keys, cache_values)
    got = exchanged(slots, KV)
    stored = [pltpu.with_memory_space_constraint(a, pltpu.HBM) for a in (cache_keys, cache_values)]
    tree, updated_keys, updated_values = pl.pallas_call(
        functools.partial(side_kernel, prop),
        out_shape=(shape(2, half, LANES), cache_keys, cache_values),
        in_specs=[SMEM, SMEM, SMEM, VMEM, VMEM, VMEM, hbm, hbm],
        out_specs=(VMEM, hbm, hbm),
        scratch_shapes=[pltpu.VMEM((2, *cache_keys.shape), bf16), pltpu.SemaphoreType.DMA((2, 2, seqs))],
        cost_estimate=pl.CostEstimate(flops=10**8, bytes_accessed=8 * MIB, transcendentals=0),
        compiler_params=pltpu.CompilerParams(vmem_limit_bytes=16 * MIB),
    )(base_length, accepted, head_bias, own, parents, fresh, *stored)
    slots = call(combine_kernel, shape(peers, half, LANES, dtype=bf16), [VMEM] * 2, 10**7, MIB, 8)(got, tree)
    got = exchanged(slots, KV)
    part = call(output_kernel, shape(rows, columns), [VMEM] * 2, 10**8, MIB, 8)(got, w_output)
    other = lax.ppermute(part, "tp", [(0, 1), (1, 0)])
    mix, slots = call(
        squares_kernel, (shape(rows, columns), shape(peers, 8, LANES)), [VMEM] * 2, 10**6, MIB // 4, 4
    )(part, other)
    got = exchanged(slots, KV)
    layer_out = call(
        functools.partial(finish_kernel, columns * peers),
        shape(rows, columns, dtype=bf16),
        [VMEM] * 2,
        10**6,
        MIB // 8,
        4,
    )(mix, got)
    return (layer_out, updated_keys, updated_values)


def solution(mesh):
    finer = Mesh(
        mesh.devices.reshape(mesh.shape["dp"], 4, 4, mesh.shape["tp"]), ("dp", "kv_0", "kv_1", "tp")
    )
    return jax.shard_map(
        shards,
        mesh=finer,
        in_specs=(
            P("dp", KV),
            P(KV),
            P(KV, "tp"),
            P(KV, "tp"),
            P(KV, "tp"),
            P(),
            P(),
            P("tp"),
            P("tp", KV),
            P("dp", KV, "tp"),
            P("dp", KV, "tp"),
            P("dp"),
            P("dp"),
            P("dp", None),
        ),
        out_specs=(P("dp", KV), P("dp", KV, "tp"), P("dp", KV, "tp")),
        check_vma=False,
    )
```

```python
import functools

import jax
import jax.numpy as jnp
from jax import lax
from jax.experimental import pallas as pl
from jax.experimental.pallas import tpu as pltpu
from jax.sharding import Mesh
from jax.sharding import PartitionSpec as P

HEAD_DIM = 64
LANES = 128
KV = ("kv_0", "kv_1")
MIB = 1 << 20
LOG2_E = 1.4426950408889634
HIDDEN = -1e30
CODE_BITS = 23.0

epsilon = 1e-05
f32 = jnp.float32
bf16 = jnp.bfloat16


def low_half(rows):
    return lax.broadcasted_iota(jnp.int32, (rows, LANES), 1) < HEAD_DIM


def turned(x):
    return pltpu.roll(x, HEAD_DIM, 1)


def dot(a, b):
    return jnp.dot(a, b, preferred_element_type=f32)


def dot_nt(a, b):
    return lax.dot_general(a, b, (((1,), (1,)), ((), ())), preferred_element_type=f32)


def split_bf16(x, pieces):
    parts = []
    for _ in range(pieces):
        part = x.astype(bf16)
        parts.append(part)
        x = x - part.astype(f32)
    return parts


def signs(z):
    spill = jnp.log(1.0 + jnp.exp(-jnp.abs(z)))
    return -jnp.maximum(z, 0.0) - spill, jnp.minimum(z, 0.0) - spill


def exits(z):
    below, above = jnp.minimum(z, 0.0), jnp.maximum(z, 0.0)
    spill = jnp.log2(1.0 + jnp.exp2(below - above))
    return above + spill, below - spill


def exponent(x):
    return jnp.ceil(jnp.log2(jnp.maximum(x, 1e-30) * 1.0001))


def coded(x, scale):
    whole = jnp.round(x * scale).astype(jnp.int32)
    return whole >> 8, whole & 255


def project_kernel(*refs):
    sources, slots, (tokens, gain, w_query, w_key, w_value), held, arrived = (
        refs[:5],
        refs[5],
        refs[6:11],
        refs[11],
        refs[12],
    )
    copies = [
        pltpu.make_async_copy(source, target, arrived.at[at])
        for at, (source, target) in enumerate(zip(sources, refs[6:11]))
    ]
    for copy in copies:
        copy.start()
    rows, half = tokens.shape[0], tokens.shape[0] // 2
    tall = rows + half
    low, low_v = low_half(rows), low_half(half)
    copies[0].wait()
    wide = tokens[...].astype(f32)
    squares = wide * wide
    squares = jnp.concatenate((squares, jnp.zeros((LANES - rows, squares.shape[1]), f32)), axis=0)
    ones = jnp.ones((8, squares.shape[1]), bf16)
    row_squares = sum(dot_nt(ones, part) for part in split_bf16(squares, 3))
    copies[1].wait()
    scaled = (wide * gain[...]).astype(bf16)
    copies[2].wait()
    copies[3].wait()
    spans = [pl.ds(at, 2 * LANES) for at in range(0, w_query.shape[1], 2 * LANES)]
    tiles = [slice(0, LANES), slice(LANES, 2 * LANES)]
    largest = jnp.zeros((rows, LANES), f32)
    for at, columns in enumerate(spans):
        query, key = dot(scaled, w_query[:, columns]), dot(scaled, w_key[:, columns])
        for tile, lanes in enumerate(tiles):
            head = 4 * at + 2 * tile
            q, k = query[:, lanes], turned(key[:, lanes])
            largest = jnp.maximum(largest, jnp.maximum(jnp.abs(q), jnp.abs(k)))
            held[head, :rows] = jnp.where(low, q, k)
            held[head + 1, :rows] = jnp.where(low, k, q)
    copies[4].wait()
    for at, columns in enumerate(spans):
        value = dot(scaled, w_value[:, columns])
        for tile, lanes in enumerate(tiles):
            head = 4 * at + 2 * tile
            v = value[:, lanes]
            largest = jnp.maximum(largest, jnp.abs(v))
            v_turned = turned(v)
            held[head, rows:] = jnp.where(low_v, v[:half], v_turned[half:])
            held[head + 1, rows:] = jnp.where(low_v, v_turned[:half], v[half:])
    power = exponent(jnp.max(largest, axis=1, keepdims=True))
    scale = jnp.broadcast_to(jnp.exp2(CODE_BITS - power), (rows, LANES))
    scale = jnp.concatenate((scale, jnp.where(low_v, scale[:half], scale[half:])), axis=0)
    lane = lax.broadcasted_iota(jnp.int32, (rows, LANES), 1)
    row = lax.broadcasted_iota(jnp.int32, (rows, LANES), 0)
    power = jnp.sum(jnp.where(lane == row, power, 0.0), axis=0, keepdims=True).astype(jnp.int32)
    square_power = exponent(row_squares)
    upper, lower = coded(row_squares, jnp.exp2(CODE_BITS - square_power))
    line = lax.broadcasted_iota(jnp.int32, (8, LANES), 0)
    notes = jnp.where(line == 0, power, jnp.where(line == 1, square_power.astype(jnp.int32), 0))
    notes = jnp.where(line == 2, upper, jnp.where(line == 3, lower, notes)).astype(jnp.int16)
    for head in range(slots.shape[0]):
        upper, lower = coded(held[head], scale)
        slots[head, :tall] = upper.astype(jnp.int16)
        both = lower[: tall // 2] * 256 + lower[tall // 2 :] - 32768
        slots[head, tall : tall + tall // 2] = both.astype(jnp.int16)
        slots[head, tall + tall // 2 :] = notes


def normalize_kernel(width, got, query_gain, key_gain, slots, own):
    peers = got.shape[0]
    tall = (got.shape[1] - 8) // 3 * 2
    half = tall // 3
    rows = 2 * half
    even = lax.axis_index(KV) % 2 == 0
    low, low_v = low_half(rows), low_half(half)
    notes = [got[peer, tall + tall // 2 :].astype(jnp.int32).astype(f32) for peer in range(peers)]
    power, square_power, upper, lower = (
        jnp.concatenate([note[line : line + 1] for note in notes], axis=0) for line in range(4)
    )
    squares = (upper * 256.0 + lower) * jnp.exp2(square_power - CODE_BITS)
    squares = jnp.sum(squares, axis=0, keepdims=True)
    scales = jnp.exp2(power - CODE_BITS)
    scales = jnp.concatenate((scales, jnp.zeros((LANES - peers, LANES), f32)), axis=0).T
    both, value = jnp.zeros((rows, LANES), f32), jnp.zeros((half, LANES), f32)
    for peer in range(peers):
        scale = jnp.broadcast_to(scales[:rows, peer : peer + 1], (rows, LANES))
        pair = got[peer, tall : tall + tall // 2].astype(jnp.int32) + 32768
        lower = jnp.concatenate((pair >> 8, pair & 255), axis=0)
        whole = (got[peer, :tall].astype(jnp.int32) * 256 + lower).astype(f32)
        both = both + whole[:rows] * scale
        value = value + whole[rows:] * jnp.where(low_v, scale[:half], scale[half:])
    power = both * both
    low_sum = jnp.sum(jnp.where(low, power, 0.0), axis=1, keepdims=True)
    high_sum = jnp.sum(jnp.where(low, 0.0, power), axis=1, keepdims=True)
    factor = lax.rsqrt(jnp.where(low, low_sum, high_sum) / HEAD_DIM + epsilon)
    one, two = query_gain[...], key_gain[...]
    gain = jnp.concatenate((jnp.where(even, one, two), jnp.where(even, two, one)), axis=1)
    normed = (both * factor * gain).astype(bf16)
    inv_rms = jnp.broadcast_to(lax.rsqrt(squares / width + epsilon), (half, LANES))
    lane = lax.broadcasted_iota(jnp.int32, (half, LANES), 1)
    row = lax.broadcasted_iota(jnp.int32, (half, LANES), 0)
    first = jnp.sum(jnp.where(lane == row, inv_rms, 0.0), axis=1, keepdims=True)
    second = jnp.sum(jnp.where(lane == row + half, inv_rms, 0.0), axis=1, keepdims=True)
    fresh = (value * jnp.where(lane < HEAD_DIM, first, second)).astype(bf16)
    own[:rows] = normed
    own[rows:] = fresh
    for peer in range(peers):
        slots[peer, :rows] = normed
        slots[peer, rows:] = fresh


def tree_part(prop, bias, own, parents, out):
    half = own.shape[0] // 3
    rows = 2 * half
    even = lax.axis_index(KV) % 2 == 0
    low = low_half(rows)
    both = own[:rows].astype(f32)
    other = turned(both)
    query = jnp.where(low, jnp.where(even, both, other), 0.0).astype(bf16)
    key = jnp.where(even, other, both).astype(bf16)
    heads = lax.broadcasted_iota(jnp.int32, bias.shape, 1)
    offset = jnp.sum(jnp.where(heads == lax.axis_index(KV), bias[...], 0.0), axis=1, keepdims=True)
    score = dot_nt(query, key) * HEAD_DIM ** (-0.5) + offset
    row = lax.broadcasted_iota(jnp.int32, (rows, rows), 0)
    column = lax.broadcasted_iota(jnp.int32, (rows, rows), 1)
    small = [lax.broadcasted_iota(jnp.int32, (prop, prop), axis) for axis in range(2)]
    parent = jnp.concatenate(
        [
            jnp.sum(jnp.where(small[0] == small[1], parents[seq : seq + 1], 0), axis=1, keepdims=True)
            for seq in range(rows // prop)
        ],
        axis=0,
    )
    direct = (parent >= 0) & (column == row - row % prop + parent)
    step = jnp.where(direct, 1.0, 0.0).astype(bf16)
    above = jnp.where(row == column, 1.0, 0.0)
    above = above + step.astype(f32)
    reach = 2
    while reach < prop:
        step = dot(step, step).astype(bf16)
        above = above + dot(above.astype(bf16), step)
        reach *= 2
    mine = (above > 0.5) & (row != column)
    stay, taken = signs(score)
    stay = jnp.where(mine, stay, 0.0)
    after = jnp.where(row > column, 1.0, 0.0).astype(bf16)
    tail = sum(dot(part, after) for part in split_bf16(stay, 3))
    weight = jnp.where(mine, jnp.exp(taken + tail), 0.0).astype(bf16)
    kept = jnp.exp(jnp.sum(stay, axis=1, keepdims=True))
    value = own[rows:].astype(f32)
    value = jnp.concatenate((value, turned(value)), axis=0).astype(bf16)
    summed = dot(weight, value)
    low = low_half(half)
    out[0] = jnp.where(low, summed[:half], turned(summed[half:]))
    out[1] = jnp.where(low, kept[:half], kept[half:])


def attend_kernel(prop, base, accepted, bias, fresh, keys, values, slots, held, sent):
    seqs, span, _ = keys.shape
    heads = fresh.shape[0]
    half = seqs * prop // 2
    group = 4
    groups = heads // group
    low = low_half(prop)
    low_mask = low.astype(f32).astype(bf16)
    high_mask = (1.0 - low.astype(f32)).astype(bf16)
    blank = jnp.zeros((prop, LANES), bf16)
    order = lax.broadcasted_iota(jnp.int32, (span, span), 0)
    after = jnp.where(order > lax.broadcasted_iota(jnp.int32, (span, span), 1), 1.0, 0.0).astype(bf16)
    position = lax.axis_index(KV) * span + lax.broadcasted_iota(jnp.int32, (1, span), 1)
    valid = base[...] + accepted[...]
    hidden = [jnp.where(position < valid[:, seq : seq + 1], 0.0, HIDDEN) for seq in range(seqs)]
    offset = bias[...] * LOG2_E
    short = prop // 2
    eighth = lax.broadcasted_iota(jnp.int32, (short, LANES), 1) // (LANES // seqs // 2)
    sending = []

    def scored(at):
        first, scores = at * group, []
        for seq in range(seqs):
            blocks = []
            for j in range(group):
                tile = fresh[first + j, seq * prop : (seq + 1) * prop] * (low_mask if j % 2 == 0 else high_mask)
                blocks.append(jnp.concatenate((tile, blank) if j < 2 else (blank, tile), axis=1))
            stored = keys[seq, :, first * HEAD_DIM : (first + group) * HEAD_DIM]
            score = dot_nt(jnp.concatenate(blocks, axis=0), stored)
            for j in range(group):
                part = score[j * prop : (j + 1) * prop]
                scores.append(part * (HEAD_DIM ** (-0.5) * LOG2_E) + (offset[:, first + j : first + j + 1] + hidden[seq]))
        return jnp.concatenate(scores, axis=0)

    def suffixes(score):
        leave, taken = exits(score)
        tall = leave.shape[0]
        tail = dot(jnp.concatenate(split_bf16(leave, 2), axis=0), after)
        tail = tail[:tall] + tail[tall:]
        log = tail[:, :1] + leave[:, :1]
        return jnp.exp2(taken - tail).astype(bf16), log

    def send(at, weight, log):
        first, tiles = at * group, []
        for seq in range(seqs):
            stored = values[seq, :, first * HEAD_DIM : (first + group) * HEAD_DIM]
            tiles.append(dot(weight[seq * group * prop : (seq + 1) * group * prop], stored))
        for j in range(group):
            head = first + j
            rows = slice(j * prop, (j + 1) * prop)
            lanes = slice(j // 2 * LANES, (j // 2 + 1) * LANES)
            for seq in range(seqs // 2):
                one, two = tiles[seq][rows, lanes], tiles[seq + seqs // 2][rows, lanes]
                one, two = (one, turned(two)) if j % 2 == 0 else (turned(one), two)
                held[head, seq * prop : (seq + 1) * prop] = jnp.where(low, one, two)
            logs = jnp.zeros((short, LANES), f32)
            for place in range(2 * seqs):
                start = (place // 2 * group + j) * prop + place % 2 * short
                logs = jnp.where(eighth == place, log[start : start + short], logs)
            held[head, half:] = logs
        chosen = pl.ds(first, group)
        copy = pltpu.make_async_copy(held.at[chosen], slots.at[chosen], sent.at[at])
        copy.start()
        sending.append(copy)

    score, ready = scored(0), None
    for at in range(groups):
        following = scored(at + 1) if at + 1 < groups else None
        weight, log = suffixes(score)
        if ready is not None:
            send(at - 1, *ready)
        ready, score = (weight, log), following
    send(groups - 1, *ready)
    for copy in sending:
        copy.wait()


def combine_kernel(got, tree, slots):
    blocks, half = got.shape[0], tree.shape[1]
    short = half // 4
    step = LANES // 8
    place = lax.broadcasted_iota(jnp.int32, (short, LANES), 1) % HEAD_DIM // step
    later = jnp.zeros((short, LANES), f32)
    part = jnp.zeros((half, LANES), f32)
    for block in range(blocks - 1, -1, -1):
        kept = jnp.exp2(-later)
        moved = {shift: kept if shift == 0 else pltpu.roll(kept, shift * step % LANES, 1) for shift in range(-3, 4)}
        pieces = []
        for wanted in range(4):
            piece = moved[-wanted]
            for at in range(1, 4):
                piece = jnp.where(place == at, moved[at - wanted], piece)
            pieces.append(piece)
        part = part + jnp.concatenate(pieces, axis=0) * got[block, :half]
        later = later + got[block, half:]
    attended = (tree[0] + tree[1] * part).astype(bf16)
    for block in range(blocks):
        slots[block] = attended


def output_kernel(got, w_output, out):
    heads, half, _ = got.shape
    low = low_half(half)
    columns = []
    for head in range(0, heads, 2):
        one, two = got[head].astype(f32), got[head + 1].astype(f32)
        top = jnp.where(low, one, turned(two))
        bottom = jnp.where(low, turned(one), two)
        columns.append(jnp.concatenate((top, bottom), axis=0).astype(bf16))
    out[...] = dot(jnp.concatenate(columns, axis=1), w_output[...])


def squares_kernel(one, two, mix, slots):
    total = one[...] + two[...]
    mix[...] = total
    rows = total.shape[0]
    squares = jnp.sum(total * total, axis=1, keepdims=True)
    lane = lax.broadcasted_iota(jnp.int32, (rows, LANES), 1)
    row = lax.broadcasted_iota(jnp.int32, (rows, LANES), 0)
    flat = jnp.sum(jnp.where(lane == row, squares, 0.0), axis=0, keepdims=True)
    slots[...] = jnp.broadcast_to(flat[None], slots.shape)


def finish_kernel(width, mix, got, out):
    total = got[0]
    for peer in range(1, got.shape[0]):
        total = total + got[peer]
    rows = out.shape[0]
    factor = jnp.broadcast_to(lax.rsqrt(total[:1] / width + epsilon), (rows, LANES))
    lane = lax.broadcasted_iota(jnp.int32, (rows, LANES), 1)
    row = lax.broadcasted_iota(jnp.int32, (rows, LANES), 0)
    factor = jnp.sum(jnp.where(lane == row, factor, 0.0), axis=1, keepdims=True)
    out[...] = (mix[...] * factor).astype(bf16)


def side_kernel(
    prop, base, accepted, bias, own, parents, fresh, keys, values, tree, new_keys, new_values, held, moved
):
    seqs, span, _ = keys.shape
    heads = fresh.shape[0]
    rows = seqs * prop
    window = 2 * prop
    loads, stores = [], []
    for seq in range(seqs):
        for which, (source, target) in enumerate(((keys, new_keys), (values, new_values))):
            block = held.at[which, seq]
            loads.append(pltpu.make_async_copy(source.at[seq], block, moved.at[0, which, seq]))
            stores.append(pltpu.make_async_copy(block, target.at[seq], moved.at[1, which, seq]))
    for copy in loads:
        copy.start()
    tree_part(prop, bias, own, parents, tree)
    valid = base[...] + accepted[...]
    low = low_half(prop)
    for seq in range(seqs):
        start = valid[0, seq] - lax.axis_index(KV) * span
        at = jnp.minimum(jnp.maximum(start, 0), span - window) // prop * prop
        lines = pl.ds(pl.multiple_of(at, prop), window)
        start = start - at
        early = seq < seqs // 2
        key_rows = slice(seq * prop, (seq + 1) * prop)
        value_rows = slice(rows + seq % (seqs // 2) * prop, rows + (seq % (seqs // 2) + 1) * prop)
        key_tiles, value_tiles = [], []
        for head in range(0, heads, 2):
            one, two = fresh[head, key_rows].astype(f32), fresh[head + 1, key_rows].astype(f32)
            key_tiles.append(turned(jnp.where(low, two, one)))
            one, two = fresh[head, value_rows].astype(f32), fresh[head + 1, value_rows].astype(f32)
            value_tiles.append(jnp.where(low, one, turned(two)) if early else jnp.where(low, turned(one), two))
        offset = lax.broadcasted_iota(jnp.int32, (window, prop), 0) - start
        chooser = jnp.where(offset == lax.broadcasted_iota(jnp.int32, (window, prop), 1), 1.0, 0.0).astype(bf16)
        offset = lax.broadcasted_iota(jnp.int32, (window, 1), 0) - start
        inside = (offset >= 0) & (offset < prop)
        for which, tiles in enumerate((key_tiles, value_tiles)):
            placed = dot(chooser, jnp.concatenate(tiles, axis=1).astype(bf16))
            loads[2 * seq + which].wait()
            old = held[which, seq, lines].astype(f32)
            held[which, seq, lines] = jnp.where(inside, placed, old).astype(bf16)
            stores[2 * seq + which].start()
    for copy in stores:
        copy.wait()


VMEM = pl.BlockSpec(memory_space=pltpu.VMEM)
SMEM = pl.BlockSpec(memory_space=pltpu.SMEM)


def call(body, outs, specs, flops, moved, limit):
    return pl.pallas_call(
        body,
        out_shape=outs,
        in_specs=specs,
        out_specs=jax.tree.map(lambda _: VMEM, outs),
        cost_estimate=pl.CostEstimate(flops=flops, bytes_accessed=moved, transcendentals=0),
        compiler_params=pltpu.CompilerParams(vmem_limit_bytes=limit * MIB),
    )


def shape(*dims, dtype=f32):
    return jax.ShapeDtypeStruct(dims, dtype)


def exchanged(slots, axis):
    return lax.all_to_all(slots, axis, 0, 0, tiled=True)


def shards(
    tokens,
    norm_gain,
    w_query,
    w_key,
    w_value,
    query_gain,
    key_gain,
    head_bias,
    w_output,
    cache_keys,
    cache_values,
    base_length,
    accepted,
    parents,
):
    seqs, prop = parents.shape
    heads = head_bias.shape[0]
    rows, span = seqs * prop, cache_keys.shape[1]
    half = rows // 2
    tall = rows + half
    columns = w_output.shape[1]
    peers = lax.axis_size(KV)
    width = tokens.shape[1] * peers
    assert peers == heads and seqs == 4 and rows <= LANES and heads % 4 == 0 and prop == 16

    lines = [a.reshape(1, -1) for a in (base_length, accepted, head_bias)]
    hbm = pl.BlockSpec(memory_space=pltpu.HBM)
    sources = [
        pltpu.with_memory_space_constraint(a, pltpu.HBM)
        for a in (tokens, norm_gain.reshape(1, -1), w_query, w_key, w_value)
    ]
    slots = pl.pallas_call(
        project_kernel,
        out_shape=pltpu.VMEM((heads, tall + tall // 2 + 8, LANES), jnp.int16),
        in_specs=[hbm] * 5,
        out_specs=VMEM,
        scratch_shapes=[pltpu.VMEM(a.shape, a.dtype) for a in sources]
        + [pltpu.VMEM((heads, tall, LANES), f32), pltpu.SemaphoreType.DMA((5,))],
        cost_estimate=pl.CostEstimate(flops=10**8, bytes_accessed=3 * MIB, transcendentals=0),
        compiler_params=pltpu.CompilerParams(vmem_limit_bytes=12 * MIB),
    )(*sources)
    got = exchanged(slots, KV)
    slots, own = call(
        functools.partial(normalize_kernel, width),
        (shape(peers, rows + half, LANES, dtype=bf16), shape(rows + half, LANES, dtype=bf16)),
        [VMEM, VMEM, VMEM],
        10**10,
        MIB,
        8,
    )(got, query_gain.reshape(1, -1), key_gain.reshape(1, -1))
    fresh = exchanged(slots, KV)
    slots = pl.pallas_call(
        functools.partial(attend_kernel, prop),
        out_shape=shape(heads, half + prop // 2, LANES),
        in_specs=[VMEM] * 6,
        out_specs=hbm,
        scratch_shapes=[pltpu.VMEM((heads, half + prop // 2, LANES), f32), pltpu.SemaphoreType.DMA((heads // 4,))],
        cost_estimate=pl.CostEstimate(flops=4 * 10**8, bytes_accessed=5 * MIB, transcendentals=0),
        compiler_params=pltpu.CompilerParams(vmem_limit_bytes=24 * MIB),
    )(*lines, fresh, cache_keys, cache_values)
    got = exchanged(slots, KV)
    stored = [pltpu.with_memory_space_constraint(a, pltpu.HBM) for a in (cache_keys, cache_values)]
    tree, updated_keys, updated_values = pl.pallas_call(
        functools.partial(side_kernel, prop),
        out_shape=(shape(2, half, LANES), cache_keys, cache_values),
        in_specs=[VMEM] * 6 + [hbm, hbm],
        out_specs=(VMEM, hbm, hbm),
        scratch_shapes=[pltpu.VMEM((2, *cache_keys.shape), bf16), pltpu.SemaphoreType.DMA((2, 2, seqs))],
        cost_estimate=pl.CostEstimate(flops=10**8, bytes_accessed=8 * MIB, transcendentals=0),
        compiler_params=pltpu.CompilerParams(vmem_limit_bytes=16 * MIB),
    )(*lines, own, parents, fresh, *stored)
    slots = call(combine_kernel, shape(peers, half, LANES, dtype=bf16), [VMEM] * 2, 10**7, MIB, 8)(got, tree)
    got = exchanged(slots, KV)
    part = call(output_kernel, shape(rows, columns), [VMEM] * 2, 10**8, MIB, 8)(got, w_output)
    other = lax.ppermute(part, "tp", [(0, 1), (1, 0)])
    mix, slots = call(
        squares_kernel, (shape(rows, columns), shape(peers, 8, LANES)), [VMEM] * 2, 10**6, MIB // 4, 4
    )(part, other)
    got = exchanged(slots, KV)
    layer_out = call(
        functools.partial(finish_kernel, columns * peers),
        shape(rows, columns, dtype=bf16),
        [VMEM] * 2,
        10**6,
        MIB // 8,
        4,
    )(mix, got)
    return (layer_out, updated_keys, updated_values)


def solution(mesh):
    finer = Mesh(
        mesh.devices.reshape(mesh.shape["dp"], 4, 4, mesh.shape["tp"]), ("dp", "kv_0", "kv_1", "tp")
    )
    return jax.shard_map(
        shards,
        mesh=finer,
        in_specs=(
            P("dp", KV),
            P(KV),
            P(KV, "tp"),
            P(KV, "tp"),
            P(KV, "tp"),
            P(),
            P(),
            P("tp"),
            P("tp", KV),
            P("dp", KV, "tp"),
            P("dp", KV, "tp"),
            P("dp"),
            P("dp"),
            P("dp", None),
        ),
        out_specs=(P("dp", KV), P("dp", KV, "tp"), P("dp", KV, "tp")),
        check_vma=False,
    )
```

```python
import functools

import jax
import jax.numpy as jnp
from jax import lax
from jax.experimental import pallas as pl
from jax.experimental.pallas import tpu as pltpu
from jax.sharding import Mesh
from jax.sharding import PartitionSpec as P

HEAD_DIM = 64
LANES = 128
KV = ("kv_0", "kv_1")
MIB = 1 << 20
LOG2_E = 1.4426950408889634
HIDDEN = -1e30
CODE_BITS = 23.0

epsilon = 1e-05
f32 = jnp.float32
bf16 = jnp.bfloat16


def low_half(rows):
    return lax.broadcasted_iota(jnp.int32, (rows, LANES), 1) < HEAD_DIM


def turned(x):
    return pltpu.roll(x, HEAD_DIM, 1)


def dot(a, b):
    return jnp.dot(a, b, preferred_element_type=f32)


def dot_nt(a, b):
    return lax.dot_general(a, b, (((1,), (1,)), ((), ())), preferred_element_type=f32)


def split_bf16(x, pieces):
    parts = []
    for _ in range(pieces):
        part = x.astype(bf16)
        parts.append(part)
        x = x - part.astype(f32)
    return parts


def signs(z):
    spill = jnp.log(1.0 + jnp.exp(-jnp.abs(z)))
    return -jnp.maximum(z, 0.0) - spill, jnp.minimum(z, 0.0) - spill


def exits(z):
    below, above = jnp.minimum(z, 0.0), jnp.maximum(z, 0.0)
    spill = jnp.log2(1.0 + jnp.exp2(below - above))
    return above + spill, below - spill


def exponent(x):
    return jnp.ceil(jnp.log2(jnp.maximum(x, 1e-30) * 1.0001))


def coded(x, scale):
    whole = jnp.round(x * scale).astype(jnp.int32)
    return whole >> 8, whole & 255


def project_kernel(*refs):
    sources, slots, (tokens, gain, w_query, w_key, w_value), held, arrived = (
        refs[:5],
        refs[5],
        refs[6:11],
        refs[11],
        refs[12],
    )
    copies = [
        pltpu.make_async_copy(source, target, arrived.at[at])
        for at, (source, target) in enumerate(zip(sources, refs[6:11]))
    ]
    for copy in copies:
        copy.start()
    rows, half = tokens.shape[0], tokens.shape[0] // 2
    tall = rows + half
    low, low_v = low_half(rows), low_half(half)
    copies[0].wait()
    wide = tokens[...].astype(f32)
    squares = wide * wide
    squares = jnp.concatenate((squares, jnp.zeros((LANES - rows, squares.shape[1]), f32)), axis=0)
    ones = jnp.ones((8, squares.shape[1]), bf16)
    row_squares = sum(dot_nt(ones, part) for part in split_bf16(squares, 3))
    copies[1].wait()
    scaled = (wide * gain[...]).astype(bf16)
    copies[2].wait()
    copies[3].wait()
    spans = [pl.ds(at, 2 * LANES) for at in range(0, w_query.shape[1], 2 * LANES)]
    tiles = [slice(0, LANES), slice(LANES, 2 * LANES)]
    largest = jnp.zeros((rows, LANES), f32)
    for at, columns in enumerate(spans):
        query, key = dot(scaled, w_query[:, columns]), dot(scaled, w_key[:, columns])
        for tile, lanes in enumerate(tiles):
            head = 4 * at + 2 * tile
            q, k = query[:, lanes], turned(key[:, lanes])
            largest = jnp.maximum(largest, jnp.maximum(jnp.abs(q), jnp.abs(k)))
            held[head, :rows] = jnp.where(low, q, k)
            held[head + 1, :rows] = jnp.where(low, k, q)
    copies[4].wait()
    for at, columns in enumerate(spans):
        value = dot(scaled, w_value[:, columns])
        for tile, lanes in enumerate(tiles):
            head = 4 * at + 2 * tile
            v = value[:, lanes]
            largest = jnp.maximum(largest, jnp.abs(v))
            v_turned = turned(v)
            held[head, rows:] = jnp.where(low_v, v[:half], v_turned[half:])
            held[head + 1, rows:] = jnp.where(low_v, v_turned[:half], v[half:])
    power = exponent(jnp.max(largest, axis=1, keepdims=True))
    scale = jnp.broadcast_to(jnp.exp2(CODE_BITS - power), (rows, LANES))
    scale = jnp.concatenate((scale, jnp.where(low_v, scale[:half], scale[half:])), axis=0)
    lane = lax.broadcasted_iota(jnp.int32, (rows, LANES), 1)
    row = lax.broadcasted_iota(jnp.int32, (rows, LANES), 0)
    power = jnp.sum(jnp.where(lane == row, power, 0.0), axis=0, keepdims=True).astype(jnp.int32)
    square_power = exponent(row_squares)
    upper, lower = coded(row_squares, jnp.exp2(CODE_BITS - square_power))
    line = lax.broadcasted_iota(jnp.int32, (8, LANES), 0)
    notes = jnp.where(line == 0, power, jnp.where(line == 1, square_power.astype(jnp.int32), 0))
    notes = jnp.where(line == 2, upper, jnp.where(line == 3, lower, notes)).astype(jnp.int16)
    for head in range(slots.shape[0]):
        upper, lower = coded(held[head], scale)
        slots[head, :tall] = upper.astype(jnp.int16)
        both = lower[: tall // 2] * 256 + lower[tall // 2 :] - 32768
        slots[head, tall : tall + tall // 2] = both.astype(jnp.int16)
        slots[head, tall + tall // 2 :] = notes


def normalize_kernel(width, got, query_gain, key_gain, slots, own):
    peers = got.shape[0]
    tall = (got.shape[1] - 8) // 3 * 2
    half = tall // 3
    rows = 2 * half
    even = lax.axis_index(KV) % 2 == 0
    low, low_v = low_half(rows), low_half(half)
    notes = [got[peer, tall + tall // 2 :].astype(jnp.int32).astype(f32) for peer in range(peers)]
    power, square_power, upper, lower = (
        jnp.concatenate([note[line : line + 1] for note in notes], axis=0) for line in range(4)
    )
    squares = (upper * 256.0 + lower) * jnp.exp2(square_power - CODE_BITS)
    squares = jnp.sum(squares, axis=0, keepdims=True)
    scales = jnp.exp2(power - CODE_BITS)
    scales = jnp.concatenate((scales, jnp.zeros((LANES - peers, LANES), f32)), axis=0).T
    both, value = jnp.zeros((rows, LANES), f32), jnp.zeros((half, LANES), f32)
    for peer in range(peers):
        scale = jnp.broadcast_to(scales[:rows, peer : peer + 1], (rows, LANES))
        pair = got[peer, tall : tall + tall // 2].astype(jnp.int32) + 32768
        lower = jnp.concatenate((pair >> 8, pair & 255), axis=0)
        whole = (got[peer, :tall].astype(jnp.int32) * 256 + lower).astype(f32)
        both = both + whole[:rows] * scale
        value = value + whole[rows:] * jnp.where(low_v, scale[:half], scale[half:])
    power = both * both
    low_sum = jnp.sum(jnp.where(low, power, 0.0), axis=1, keepdims=True)
    high_sum = jnp.sum(jnp.where(low, 0.0, power), axis=1, keepdims=True)
    factor = lax.rsqrt(jnp.where(low, low_sum, high_sum) / HEAD_DIM + epsilon)
    one, two = query_gain[...], key_gain[...]
    gain = jnp.concatenate((jnp.where(even, one, two), jnp.where(even, two, one)), axis=1)
    normed = (both * factor * gain).astype(bf16)
    inv_rms = jnp.broadcast_to(lax.rsqrt(squares / width + epsilon), (half, LANES))
    lane = lax.broadcasted_iota(jnp.int32, (half, LANES), 1)
    row = lax.broadcasted_iota(jnp.int32, (half, LANES), 0)
    first = jnp.sum(jnp.where(lane == row, inv_rms, 0.0), axis=1, keepdims=True)
    second = jnp.sum(jnp.where(lane == row + half, inv_rms, 0.0), axis=1, keepdims=True)
    fresh = (value * jnp.where(lane < HEAD_DIM, first, second)).astype(bf16)
    own[:rows] = normed
    own[rows:] = fresh
    for peer in range(peers):
        slots[peer, :rows] = normed
        slots[peer, rows:] = fresh


def tree_part(prop, bias, own, parents, out):
    half = own.shape[0] // 3
    rows = 2 * half
    even = lax.axis_index(KV) % 2 == 0
    low = low_half(rows)
    both = own[:rows].astype(f32)
    other = turned(both)
    query = jnp.where(low, jnp.where(even, both, other), 0.0).astype(bf16)
    key = jnp.where(even, other, both).astype(bf16)
    heads = lax.broadcasted_iota(jnp.int32, bias.shape, 1)
    offset = jnp.sum(jnp.where(heads == lax.axis_index(KV), bias[...], 0.0), axis=1, keepdims=True)
    score = dot_nt(query, key) * HEAD_DIM ** (-0.5) + offset
    row = lax.broadcasted_iota(jnp.int32, (rows, rows), 0)
    column = lax.broadcasted_iota(jnp.int32, (rows, rows), 1)
    small = [lax.broadcasted_iota(jnp.int32, (prop, prop), axis) for axis in range(2)]
    parent = jnp.concatenate(
        [
            jnp.sum(jnp.where(small[0] == small[1], parents[seq : seq + 1], 0), axis=1, keepdims=True)
            for seq in range(rows // prop)
        ],
        axis=0,
    )
    direct = (parent >= 0) & (column == row - row % prop + parent)
    step = jnp.where(direct, 1.0, 0.0).astype(bf16)
    above = jnp.where(row == column, 1.0, 0.0)
    above = above + step.astype(f32)
    reach = 2
    while reach < prop:
        step = dot(step, step).astype(bf16)
        above = above + dot(above.astype(bf16), step)
        reach *= 2
    mine = (above > 0.5) & (row != column)
    stay, taken = signs(score)
    stay = jnp.where(mine, stay, 0.0)
    after = jnp.where(row > column, 1.0, 0.0).astype(bf16)
    tail = sum(dot(part, after) for part in split_bf16(stay, 3))
    weight = jnp.where(mine, jnp.exp(taken + tail), 0.0).astype(bf16)
    kept = jnp.exp(jnp.sum(stay, axis=1, keepdims=True))
    value = own[rows:].astype(f32)
    value = jnp.concatenate((value, turned(value)), axis=0).astype(bf16)
    summed = dot(weight, value)
    low = low_half(half)
    out[0] = jnp.where(low, summed[:half], turned(summed[half:]))
    out[1] = jnp.where(low, kept[:half], kept[half:])


def attend_kernel(prop, base, accepted, bias, fresh, keys, values, slots, held, sent):
    seqs, span, _ = keys.shape
    heads = fresh.shape[0]
    half = seqs * prop // 2
    group = 4
    groups = heads // group
    low = low_half(prop)
    low_mask = low.astype(f32).astype(bf16)
    high_mask = (1.0 - low.astype(f32)).astype(bf16)
    blank = jnp.zeros((prop, LANES), bf16)
    order = lax.broadcasted_iota(jnp.int32, (span, span), 0)
    after = jnp.where(order > lax.broadcasted_iota(jnp.int32, (span, span), 1), 1.0, 0.0).astype(bf16)
    position = lax.axis_index(KV) * span + lax.broadcasted_iota(jnp.int32, (1, span), 1)
    valid = base[...] + accepted[...]
    hidden = [jnp.where(position < valid[:, seq : seq + 1], 0.0, HIDDEN) for seq in range(seqs)]
    offset = bias[...] * LOG2_E
    short = prop // 2
    eighth = lax.broadcasted_iota(jnp.int32, (short, LANES), 1) // (LANES // seqs // 2)
    sending = []

    def scored(at):
        first, scores = at * group, []
        for seq in range(seqs):
            blocks = []
            for j in range(group):
                tile = fresh[first + j, seq * prop : (seq + 1) * prop] * (low_mask if j % 2 == 0 else high_mask)
                blocks.append(jnp.concatenate((tile, blank) if j < 2 else (blank, tile), axis=1))
            stored = keys[seq, :, first * HEAD_DIM : (first + group) * HEAD_DIM]
            score = dot_nt(jnp.concatenate(blocks, axis=0), stored)
            for j in range(group):
                part = score[j * prop : (j + 1) * prop]
                scores.append(part * (HEAD_DIM ** (-0.5) * LOG2_E) + (offset[:, first + j : first + j + 1] + hidden[seq]))
        return jnp.concatenate(scores, axis=0)

    def suffixes(score):
        leave, taken = exits(score)
        tall = leave.shape[0]
        tail = dot(jnp.concatenate(split_bf16(leave, 2), axis=0), after)
        tail = tail[:tall] + tail[tall:]
        log = tail[:, :1] + leave[:, :1]
        return jnp.exp2(taken - tail).astype(bf16), log

    def send(at, weight, log):
        first, tiles = at * group, []
        for seq in range(seqs):
            stored = values[seq, :, first * HEAD_DIM : (first + group) * HEAD_DIM]
            tiles.append(dot(weight[seq * group * prop : (seq + 1) * group * prop], stored))
        for j in range(group):
            head = first + j
            rows = slice(j * prop, (j + 1) * prop)
            lanes = slice(j // 2 * LANES, (j // 2 + 1) * LANES)
            for seq in range(seqs // 2):
                one, two = tiles[seq][rows, lanes], tiles[seq + seqs // 2][rows, lanes]
                one, two = (one, turned(two)) if j % 2 == 0 else (turned(one), two)
                held[head, seq * prop : (seq + 1) * prop] = jnp.where(low, one, two)
            logs = jnp.zeros((short, LANES), f32)
            for place in range(2 * seqs):
                start = (place // 2 * group + j) * prop + place % 2 * short
                logs = jnp.where(eighth == place, log[start : start + short], logs)
            held[head, half:] = logs
        chosen = pl.ds(first, group)
        copy = pltpu.make_async_copy(held.at[chosen], slots.at[chosen], sent.at[at])
        copy.start()
        sending.append(copy)

    score, ready = scored(0), None
    for at in range(groups):
        following = scored(at + 1) if at + 1 < groups else None
        weight, log = suffixes(score)
        if ready is not None:
            send(at - 1, *ready)
        ready, score = (weight, log), following
    send(groups - 1, *ready)
    for copy in sending:
        copy.wait()


def combine_kernel(got, tree, slots):
    blocks, half = got.shape[0], tree.shape[1]
    short = half // 4
    step = LANES // 8
    place = lax.broadcasted_iota(jnp.int32, (short, LANES), 1) % HEAD_DIM // step
    later = jnp.zeros((short, LANES), f32)
    part = jnp.zeros((half, LANES), f32)
    for block in range(blocks - 1, -1, -1):
        kept = jnp.exp2(-later)
        moved = {shift: kept if shift == 0 else pltpu.roll(kept, shift * step % LANES, 1) for shift in range(-3, 4)}
        pieces = []
        for wanted in range(4):
            piece = moved[-wanted]
            for at in range(1, 4):
                piece = jnp.where(place == at, moved[at - wanted], piece)
            pieces.append(piece)
        part = part + jnp.concatenate(pieces, axis=0) * got[block, :half]
        later = later + got[block, half:]
    attended = (tree[0] + tree[1] * part).astype(bf16)
    for block in range(blocks):
        slots[block] = attended


def output_kernel(got, w_output, out):
    heads, half, _ = got.shape
    low = low_half(half)
    columns = []
    for head in range(0, heads, 2):
        one, two = got[head].astype(f32), got[head + 1].astype(f32)
        top = jnp.where(low, one, turned(two))
        bottom = jnp.where(low, turned(one), two)
        columns.append(jnp.concatenate((top, bottom), axis=0).astype(bf16))
    out[...] = dot(jnp.concatenate(columns, axis=1), w_output[...])


def squares_kernel(one, two, mix, slots):
    total = one[...] + two[...]
    mix[...] = total
    rows = total.shape[0]
    squares = jnp.sum(total * total, axis=1, keepdims=True)
    lane = lax.broadcasted_iota(jnp.int32, (rows, LANES), 1)
    row = lax.broadcasted_iota(jnp.int32, (rows, LANES), 0)
    flat = jnp.sum(jnp.where(lane == row, squares, 0.0), axis=0, keepdims=True)
    slots[...] = jnp.broadcast_to(flat[None], slots.shape)


def finish_kernel(width, mix, got, out):
    total = got[0]
    for peer in range(1, got.shape[0]):
        total = total + got[peer]
    rows = out.shape[0]
    factor = jnp.broadcast_to(lax.rsqrt(total[:1] / width + epsilon), (rows, LANES))
    lane = lax.broadcasted_iota(jnp.int32, (rows, LANES), 1)
    row = lax.broadcasted_iota(jnp.int32, (rows, LANES), 0)
    factor = jnp.sum(jnp.where(lane == row, factor, 0.0), axis=1, keepdims=True)
    out[...] = (mix[...] * factor).astype(bf16)


def side_kernel(
    prop, base, accepted, bias, own, parents, fresh, keys, values, tree, new_keys, new_values, held, moved
):
    seqs, span, _ = keys.shape
    heads = fresh.shape[0]
    rows = seqs * prop
    window = 2 * prop
    loads, stores = [], []
    for seq in range(seqs):
        for which, (source, target) in enumerate(((keys, new_keys), (values, new_values))):
            block = held.at[which, seq]
            loads.append(pltpu.make_async_copy(source.at[seq], block, moved.at[0, which, seq]))
            stores.append(pltpu.make_async_copy(block, target.at[seq], moved.at[1, which, seq]))
    for copy in loads:
        copy.start()
    tree_part(prop, bias, own, parents, tree)
    valid = base[...] + accepted[...]
    low = low_half(prop)
    for seq in range(seqs):
        start = valid[0, seq] - lax.axis_index(KV) * span
        at = jnp.minimum(jnp.maximum(start, 0), span - window) // prop * prop
        lines = pl.ds(pl.multiple_of(at, prop), window)
        start = start - at
        early = seq < seqs // 2
        key_rows = slice(seq * prop, (seq + 1) * prop)
        value_rows = slice(rows + seq % (seqs // 2) * prop, rows + (seq % (seqs // 2) + 1) * prop)
        key_tiles, value_tiles = [], []
        for head in range(0, heads, 2):
            one, two = fresh[head, key_rows].astype(f32), fresh[head + 1, key_rows].astype(f32)
            key_tiles.append(turned(jnp.where(low, two, one)))
            one, two = fresh[head, value_rows].astype(f32), fresh[head + 1, value_rows].astype(f32)
            value_tiles.append(jnp.where(low, one, turned(two)) if early else jnp.where(low, turned(one), two))
        offset = lax.broadcasted_iota(jnp.int32, (window, prop), 0) - start
        chooser = jnp.where(offset == lax.broadcasted_iota(jnp.int32, (window, prop), 1), 1.0, 0.0).astype(bf16)
        offset = lax.broadcasted_iota(jnp.int32, (window, 1), 0) - start
        inside = (offset >= 0) & (offset < prop)
        for which, tiles in enumerate((key_tiles, value_tiles)):
            placed = dot(chooser, jnp.concatenate(tiles, axis=1).astype(bf16))
            loads[2 * seq + which].wait()
            old = held[which, seq, lines].astype(f32)
            held[which, seq, lines] = jnp.where(inside, placed, old).astype(bf16)
            stores[2 * seq + which].start()
    for copy in stores:
        copy.wait()


VMEM = pl.BlockSpec(memory_space=pltpu.VMEM)
SMEM = pl.BlockSpec(memory_space=pltpu.SMEM)


def call(body, outs, specs, flops, moved, limit):
    return pl.pallas_call(
        body,
        out_shape=outs,
        in_specs=specs,
        out_specs=jax.tree.map(lambda _: VMEM, outs),
        cost_estimate=pl.CostEstimate(flops=flops, bytes_accessed=moved, transcendentals=0),
        compiler_params=pltpu.CompilerParams(vmem_limit_bytes=limit * MIB),
    )


def shape(*dims, dtype=f32):
    return jax.ShapeDtypeStruct(dims, dtype)


def exchanged(slots, axis):
    return lax.all_to_all(slots, axis, 0, 0, tiled=True)


def shards(
    tokens,
    norm_gain,
    w_query,
    w_key,
    w_value,
    query_gain,
    key_gain,
    head_bias,
    w_output,
    cache_keys,
    cache_values,
    base_length,
    accepted,
    parents,
):
    seqs, prop = parents.shape
    heads = head_bias.shape[0]
    rows, span = seqs * prop, cache_keys.shape[1]
    half = rows // 2
    tall = rows + half
    columns = w_output.shape[1]
    peers = lax.axis_size(KV)
    width = tokens.shape[1] * peers
    assert peers == heads and seqs == 4 and rows <= LANES and heads % 4 == 0 and prop == 16

    lines = [a.reshape(1, -1) for a in (base_length, accepted, head_bias)]
    hbm = pl.BlockSpec(memory_space=pltpu.HBM)
    sources = [
        pltpu.with_memory_space_constraint(a, pltpu.HBM)
        for a in (tokens, norm_gain.reshape(1, -1), w_query, w_key, w_value)
    ]
    slots = pl.pallas_call(
        project_kernel,
        out_shape=pltpu.VMEM((heads, tall + tall // 2 + 8, LANES), jnp.int16),
        in_specs=[hbm] * 5,
        out_specs=VMEM,
        scratch_shapes=[pltpu.VMEM(a.shape, a.dtype) for a in sources]
        + [pltpu.VMEM((heads, tall, LANES), f32), pltpu.SemaphoreType.DMA((5,))],
        cost_estimate=pl.CostEstimate(flops=10**8, bytes_accessed=3 * MIB, transcendentals=0),
        compiler_params=pltpu.CompilerParams(vmem_limit_bytes=12 * MIB),
    )(*sources)
    got = exchanged(slots, KV)
    slots, own = call(
        functools.partial(normalize_kernel, width),
        (shape(peers, rows + half, LANES, dtype=bf16), shape(rows + half, LANES, dtype=bf16)),
        [VMEM, VMEM, VMEM],
        10**10,
        MIB,
        8,
    )(got, query_gain.reshape(1, -1), key_gain.reshape(1, -1))
    fresh = exchanged(slots, KV)
    slots = pl.pallas_call(
        functools.partial(attend_kernel, prop),
        out_shape=shape(heads, half + prop // 2, LANES),
        in_specs=[VMEM] * 6,
        out_specs=hbm,
        scratch_shapes=[pltpu.VMEM((heads, half + prop // 2, LANES), f32), pltpu.SemaphoreType.DMA((heads // 4,))],
        cost_estimate=pl.CostEstimate(flops=4 * 10**8, bytes_accessed=5 * MIB, transcendentals=0),
        compiler_params=pltpu.CompilerParams(vmem_limit_bytes=24 * MIB),
    )(*lines, fresh, cache_keys, cache_values)
    got = exchanged(slots, KV)
    stored = [pltpu.with_memory_space_constraint(a, pltpu.HBM) for a in (cache_keys, cache_values)]
    tree, updated_keys, updated_values = pl.pallas_call(
        functools.partial(side_kernel, prop),
        out_shape=(shape(2, half, LANES), cache_keys, cache_values),
        in_specs=[VMEM] * 6 + [hbm, hbm],
        out_specs=(VMEM, hbm, hbm),
        scratch_shapes=[pltpu.VMEM((2, *cache_keys.shape), bf16), pltpu.SemaphoreType.DMA((2, 2, seqs))],
        cost_estimate=pl.CostEstimate(flops=10**8, bytes_accessed=8 * MIB, transcendentals=0),
        compiler_params=pltpu.CompilerParams(vmem_limit_bytes=16 * MIB),
    )(*lines, own, parents, fresh, *stored)
    slots = call(combine_kernel, shape(peers, half, LANES, dtype=bf16), [VMEM] * 2, 10**7, MIB, 8)(got, tree)
    got = exchanged(slots, KV)
    part = call(output_kernel, shape(rows, columns), [VMEM] * 2, 10**8, MIB, 8)(got, w_output)
    other = lax.ppermute(part, "tp", [(0, 1), (1, 0)])
    mix, slots = call(
        squares_kernel, (shape(rows, columns), shape(peers, 1, LANES)), [VMEM] * 2, 10**6, MIB // 4, 4
    )(part, other)
    got = exchanged(slots, KV)
    layer_out = call(
        functools.partial(finish_kernel, columns * peers),
        shape(rows, columns, dtype=bf16),
        [VMEM] * 2,
        10**6,
        MIB // 8,
        4,
    )(mix, got)
    return (layer_out, updated_keys, updated_values)


def solution(mesh):
    finer = Mesh(
        mesh.devices.reshape(mesh.shape["dp"], 4, 4, mesh.shape["tp"]), ("dp", "kv_0", "kv_1", "tp")
    )
    return jax.shard_map(
        shards,
        mesh=finer,
        in_specs=(
            P("dp", KV),
            P(KV),
            P(KV, "tp"),
            P(KV, "tp"),
            P(KV, "tp"),
            P(),
            P(),
            P("tp"),
            P("tp", KV),
            P("dp", KV, "tp"),
            P("dp", KV, "tp"),
            P("dp"),
            P("dp"),
            P("dp", None),
        ),
        out_specs=(P("dp", KV), P("dp", KV, "tp"), P("dp", KV, "tp")),
        check_vma=False,
    )
```
